32 devices in a mesh: sp: 16 (over z, y, core), tp: 2 (over x).
Axes of the slice: x: 2, y: 2, z: 4, core: 2. Of those that a mesh axis runs over, the one named last changes fastest.
Arguments:
- queries: bfloat16 [4096, 512], P('sp', 'tp'), may hold values from -8 to 8
- keys: bfloat16 [4096, 512], P('sp', 'tp'), may hold values from -8 to 8
- values: bfloat16 [4096, 512], P('sp', 'tp'), may hold values from -6 to 6
- score_shift: float32 [8], P('tp'), may hold values from 3 to 20
- resid: bfloat16 [4096, 2048], P(('sp', 'tp')), may hold values from -6 to 6
- w_out: bfloat16 [512, 2048], replicated, may hold values from -0.25 to 0.25
- gain_mix: float32 [2048], replicated, may hold values from 0.1 to 1.9
- gain_pre: float32 [2048], replicated, may hold values from 0.1 to 1.9
- w_gate: bfloat16 [2048, 5632], P('sp', 'tp'), may hold values from -0.125 to 0.125
- w_up: bfloat16 [2048, 5632], P('sp', 'tp'), may hold values from -0.125 to 0.125
- conv_gate: float32 [3, 5632], P(None, 'tp'), may hold values from -3 to 3
- conv_up: float32 [3, 5632], P(None, 'tp'), may hold values from -3 to 3
- w_down: bfloat16 [5632, 2048], P('tp', 'sp'), may hold values from -0.078125 to 0.078125
- gain_post: float32 [2048], replicated, may hold values from 0.1 to 1.9
Outputs:
- result: bfloat16 [4096, 2048], P(('sp', 'tp'))
The draws below stay inside these ranges and needn't reach their ends.
All inputs are finite; a program needn't handle non-finite values.
Results may differ from the reference program's by a relative error of at most 0.017.
Values may be sent and summed in bfloat16 or wider, within the bound.
A program may use at most 128 MiB of HBM per device.

```python
import math
import jax
import jax.numpy as jnp
from jax import lax

D = 2048
HEADS = 8
HEAD_DIM = 64
FF = 5632
KERNEL = 3
SEQ = 4096
N_TP = 2


def level_of(rng, dims, split, low, top_value):
    gain, own = 1.0, jax.random.fold_in(rng, 6)
    for axis_at, parts in split:
        heights = jnp.exp(jax.random.uniform(jax.random.fold_in(own, axis_at), (parts,), jnp.float32, low / len(split), top_value / len(split)))
        gain = gain * jnp.repeat(heights, dims[axis_at] // parts).reshape([-1 if axis == axis_at else 1 for axis in range(len(dims))])
    return gain


def scatter_about(key, dims, deviation, limit, shards=(), kind=jnp.bfloat16):
    factor_of = level_of(key, dims, shards, -0.22, 0.18) if shards else 1.0
    values = jax.random.normal(key, dims, jnp.float32) * deviation * factor_of
    return jnp.minimum(jnp.maximum(values, -limit), limit).astype(kind)


def setup_inputs(seed: int = 0) -> dict:
    arg_keys = jax.random.split(jax.random.key(seed), 15)
    queries = scatter_about(arg_keys[0], (SEQ, HEADS * HEAD_DIM), 2.0, 8.0, ((0, 16), (1, 2)))
    keys = scatter_about(arg_keys[1], (SEQ, HEADS * HEAD_DIM), 2.0, 8.0, ((0, 16), (1, 2)))
    values = scatter_about(arg_keys[2], (SEQ, HEADS * HEAD_DIM), 1.0, 6.0, ((0, 16), (1, 2)))
    score_shift = jnp.clip(jnp.exp(math.log(20.0) - 1.89712 * jax.random.uniform(arg_keys[3], (HEADS,), jnp.float32) ** level_of(arg_keys[3], (HEADS,), ((0, 2),), -0.2, 0.2)), 3.0, 20.0)
    resid = scatter_about(arg_keys[4], (SEQ, D), 1.0, 6.0, ((0, 32),))
    w_out = scatter_about(arg_keys[5], (HEADS * HEAD_DIM, D), (HEADS * HEAD_DIM) ** -0.5, 0.25)
    gain_mix = jnp.clip(1.0 + 0.18 * jax.random.normal(arg_keys[6], (D,), jnp.float32), 0.1, 1.9)
    gain_pre = jnp.clip(1.0 + 0.18 * jax.random.normal(arg_keys[7], (D,), jnp.float32), 0.1, 1.9)
    w_gate = scatter_about(arg_keys[8], (D, FF), D ** -0.5, 0.125, ((0, 16), (1, 2)))
    w_up = scatter_about(arg_keys[9], (D, FF), D ** -0.5, 0.125, ((0, 16), (1, 2)))
    conv_gate = scatter_about(arg_keys[10], (KERNEL, FF), 0.577, 3.0, ((1, 2),), jnp.float32)
    conv_up = scatter_about(arg_keys[11], (KERNEL, FF), 0.577, 3.0, ((1, 2),), jnp.float32)
    w_down = scatter_about(arg_keys[12], (FF, D), FF ** -0.5, 0.078125, ((0, 2), (1, 16)))
    gain_post = jnp.clip(1.0 + 0.18 * jax.random.normal(arg_keys[13], (D,), jnp.float32), 0.1, 1.9)
    return dict(queries=queries, keys=keys, values=values, score_shift=score_shift, resid=resid, w_out=w_out, gain_mix=gain_mix, gain_pre=gain_pre, w_gate=w_gate, w_up=w_up, conv_gate=conv_gate, conv_up=conv_up, w_down=w_down, gain_post=gain_post)


def rms_scale(values_in):
    return values_in * lax.rsqrt(lax.optimization_barrier(jnp.mean(values_in * values_in, axis=-1, keepdims=True)) + 1e-06)

def stick_attention(queries, keys, values, score_shift):
    length = queries.shape[0]
    query_heads = queries.reshape(length, HEADS, HEAD_DIM).transpose(1, 0, 2)
    key_heads = keys.reshape(length, HEADS, HEAD_DIM).transpose(1, 0, 2)
    value_heads = values.reshape(length, HEADS, HEAD_DIM).transpose(1, 0, 2)
    block = math.gcd(length, 512)
    blocks = length // block
    key_pos = jnp.arange(length, dtype=jnp.int32)

    def one_block(index):
        head = index // blocks
        first = index % blocks * block
        query_block = lax.dynamic_slice(query_heads, (head, first, jnp.int32(0)), (1, block, HEAD_DIM))[0]
        key_head = lax.dynamic_index_in_dim(key_heads, head, 0, keepdims=False)
        value_head = lax.dynamic_index_in_dim(value_heads, head, 0, keepdims=False)
        shift = lax.dynamic_index_in_dim(score_shift, head, 0, keepdims=False)
        scores = jnp.dot(query_block, key_head.T, preferred_element_type=jnp.float32) * HEAD_DIM ** (-0.5) - shift
        query_pos = first + jnp.arange(block, dtype=jnp.int32)
        causal = key_pos[None, :] < query_pos[:, None]
        log_keep = jnp.where(causal, -jax.nn.softplus(scores), 0.0)
        later = lax.cumsum(log_keep, axis=1, reverse=True) - log_keep
        weights = jnp.where(causal, jnp.exp(jax.nn.log_sigmoid(scores) + later), 0.0).astype(jnp.bfloat16)
        return jnp.dot(weights, value_head, preferred_element_type=jnp.float32).astype(jnp.bfloat16)
    outputs = lax.map(one_block, jnp.arange(HEADS * blocks, dtype=jnp.int32))
    outputs = outputs.reshape(HEADS, length, HEAD_DIM)
    return outputs.transpose(1, 0, 2).reshape(length, HEADS * HEAD_DIM)

def reference(queries, keys, values, score_shift, resid, w_out, gain_mix, gain_pre, w_gate, w_up, conv_gate, conv_up, w_down, gain_post):
    attended = stick_attention(queries, keys, values, score_shift)
    mixed = jnp.dot(attended, w_out, preferred_element_type=jnp.float32).astype(jnp.bfloat16)
    middle = (resid.astype(jnp.float32) + gain_mix * rms_scale(mixed.astype(jnp.float32))).astype(jnp.bfloat16)
    normed = (gain_pre * rms_scale(middle.astype(jnp.float32))).astype(jnp.bfloat16)
    gate_proj = jnp.dot(normed, w_gate, preferred_element_type=jnp.float32).astype(jnp.bfloat16)
    up_proj = jnp.dot(normed, w_up, preferred_element_type=jnp.float32).astype(jnp.bfloat16)
    length = normed.shape[0]
    gate_pad = jnp.pad(gate_proj.astype(jnp.float32), ((KERNEL - 1, 0), (0, 0)))
    up_pad = jnp.pad(up_proj.astype(jnp.float32), ((KERNEL - 1, 0), (0, 0)))
    gate_conv = jnp.zeros((length, FF), jnp.float32)
    up_conv = jnp.zeros((length, FF), jnp.float32)
    for tap in range(KERNEL):
        gate_conv = gate_conv + conv_gate[tap] * gate_pad[tap:tap + length]
        up_conv = up_conv + conv_up[tap] * up_pad[tap:tap + length]
    hidden = (jax.nn.silu(gate_conv) * up_conv).astype(jnp.bfloat16)
    width_block = FF // N_TP
    summed = jnp.zeros((length, D), jnp.float32)
    for index in range(N_TP):
        partial_sum = jnp.dot(hidden[:, index * width_block:(index + 1) * width_block], w_down[index * width_block:(index + 1) * width_block], preferred_element_type=jnp.float32)
        summed = summed + partial_sum.astype(jnp.bfloat16).astype(jnp.float32)
    ffn_out = summed.astype(jnp.bfloat16)
    return (middle.astype(jnp.float32) + gain_post * rms_scale(ffn_out.astype(jnp.float32))).astype(jnp.bfloat16)
```

```python
import functools

import jax
import jax.numpy as jnp
from jax import lax
from jax.experimental import pallas as pl
from jax.experimental.pallas import tpu as pltpu
from jax.sharding import PartitionSpec as P

HEAD_DIM = 64
KERNEL = 3


def from_behind(x, axis, by):
    length = lax.axis_size(axis)
    pairs = [(i, i + by) for i in range(length) if 0 <= i + by < length]
    return lax.ppermute(x, axis, pairs)


def rms_scale(values_in):
    return values_in * lax.rsqrt(jnp.mean(values_in * values_in, axis=-1, keepdims=True) + 1e-06)


def collect_weights(w_gate, w_up, w_down):
    gate_whole, up_whole = (
        lax.all_gather(w_gate, "sp", axis=0, tiled=True),
        lax.all_gather(w_up, "sp", axis=0, tiled=True),
    )
    down_whole = lax.all_gather(w_down, "sp", axis=1, tiled=True)
    return (gate_whole, up_whole, down_whole)


def stick_attention(queries, key_whole, value_whole, score_shift):
    tok_rows = queries.shape[0]
    local_heads = queries.shape[1] // HEAD_DIM
    total = key_whole.shape[0]
    shards = total // tok_rows
    group = max(
        (
            factor
            for factor in range(1, shards + 1)
            if shards % factor == 0 and factor * tok_rows <= max(2048, tok_rows)
        )
    )
    span = group * tok_rows
    offset = lax.axis_index("sp") * tok_rows
    query_heads = queries.reshape(tok_rows, local_heads, HEAD_DIM)
    key_heads = key_whole.reshape(total, local_heads, HEAD_DIM)
    value_heads = value_whole.reshape(total, local_heads, HEAD_DIM)
    query_pos = offset + jnp.arange(tok_rows, dtype=jnp.int32)
    last_block = (offset + tok_rows - 1) // span

    def visit(turn, carry):
        accum, tail = carry
        block_start = (last_block - turn) * span
        key_block = lax.dynamic_slice_in_dim(key_heads, block_start, span, 0)
        value_block = lax.dynamic_slice_in_dim(value_heads, block_start, span, 0)
        scores = jnp.einsum(
            "qhd,khd->hqk", query_heads, key_block, preferred_element_type=jnp.float32
        )
        scores = scores * HEAD_DIM ** (-0.5) - score_shift[:, None, None]
        key_pos = block_start + jnp.arange(span, dtype=jnp.int32)
        causal = (key_pos[None, :] < query_pos[:, None])[None, :, :]
        log_keep = jnp.where(causal, -jax.nn.softplus(scores), 0.0)
        later = lax.cumsum(log_keep, axis=2, reverse=True) - log_keep
        weights = jnp.where(
            causal, jnp.exp(jax.nn.log_sigmoid(scores) + later + tail[:, :, None]), 0.0
        ).astype(jnp.bfloat16)
        accum = accum + jnp.einsum(
            "hqk,khd->hqd", weights, value_block, preferred_element_type=jnp.float32
        )
        return (accum, tail + jnp.sum(log_keep, axis=2))

    start_carry = (
        jnp.zeros((local_heads, tok_rows, HEAD_DIM), jnp.float32),
        jnp.zeros((local_heads, tok_rows), jnp.float32),
    )
    accum, _ = lax.fori_loop(0, last_block + 1, visit, start_carry)
    return accum.transpose(1, 0, 2).reshape(tok_rows, local_heads * HEAD_DIM).astype(jnp.bfloat16)


def generic_local(
    queries,
    keys,
    values,
    score_shift,
    resid,
    w_out,
    gain_mix,
    gain_pre,
    w_gate,
    w_up,
    conv_gate,
    conv_up,
    w_down,
    gain_post,
):
    gate_whole, up_whole, down_whole = collect_weights(w_gate, w_up, w_down)
    key_whole, value_whole = (
        lax.all_gather(keys, "sp", axis=0, tiled=True),
        lax.all_gather(values, "sp", axis=0, tiled=True),
    )
    attended = stick_attention(queries, key_whole, value_whole, score_shift)
    head_rows = lax.all_to_all(attended, "tp", split_axis=0, concat_axis=1, tiled=True)
    mixed = jnp.dot(head_rows, w_out, preferred_element_type=jnp.float32).astype(jnp.bfloat16)
    middle = (resid.astype(jnp.float32) + gain_mix * rms_scale(mixed.astype(jnp.float32))).astype(
        jnp.bfloat16
    )
    normed = (gain_pre * rms_scale(middle.astype(jnp.float32))).astype(jnp.bfloat16)
    piece = lax.all_gather(normed, "tp", axis=0, tiled=True)
    gate_part = jnp.dot(piece, gate_whole, preferred_element_type=jnp.float32).astype(jnp.bfloat16)
    up_part = jnp.dot(piece, up_whole, preferred_element_type=jnp.float32).astype(jnp.bfloat16)
    projected = jnp.concatenate([gate_part, up_part], axis=1)
    tok_rows = projected.shape[0]
    local_units = projected.shape[1] // 2
    edge = from_behind(projected[tok_rows - (KERNEL - 1) :], "sp", 1)
    extended = jnp.concatenate([edge, projected], axis=0).astype(jnp.float32)
    taps = jnp.concatenate([conv_gate, conv_up], axis=1)
    convolved = taps[0] * extended[0:tok_rows]
    for tap in range(1, KERNEL):
        convolved = convolved + taps[tap] * extended[tap : tap + tok_rows]
    hidden = (jax.nn.silu(convolved[:, :local_units]) * convolved[:, local_units:]).astype(
        jnp.bfloat16
    )
    summed = lax.psum_scatter(
        jnp.dot(hidden, down_whole, preferred_element_type=jnp.float32).astype(jnp.bfloat16),
        "tp",
        scatter_dimension=0,
        tiled=True,
    )
    return (middle.astype(jnp.float32) + gain_post * rms_scale(summed.astype(jnp.float32))).astype(
        jnp.bfloat16
    )


MESH = pl.DeviceIdType.MESH
NZ, NY, NC = 4, 2, 2


def front_kernel(
    q_ref, k_ref, v_ref, shift_ref, wg_ref, wu_ref, wd_ref,
    att_ref, gate_ref, up_ref, down_ref,
    kbuf, vbuf, qs, acc, tail, tri, own_g, own_u, own_d,
    kv_send, kv_recv, w_send, w_recv, loc_in, loc_out,
):
    rows, width = q_ref.shape
    heads = width // HEAD_DIM
    depth = wg_ref.shape[0]
    units = gate_ref.shape[1]
    cols = wd_ref.shape[1]
    sp = lax.axis_index("sp")
    z, y, c = sp // (NY * NC), (sp // NC) % NY, sp % NC
    half = z // 2
    inner = (z == 1) | (z == 2)
    cross_in = 2 - half
    cross_out = 3 - 3 * half
    z_mate = z + 1 - 2 * lax.rem(z, 2)

    def dev(zz, yy, cc):
        return (zz * NY + yy) * NC + cc

    y_dev, c_dev, m_dev = dev(z, 1 - y, c), dev(z, y, 1 - c), dev(z_mate, y, c)

    def remote(src, dst, ssem, rsem, target):
        return pltpu.make_async_remote_copy(
            src_ref=src, dst_ref=dst, send_sem=ssem, recv_sem=rsem,
            device_id={"sp": target}, device_id_type=MESH,
        )

    own = (own_g, own_u, own_d)
    loads = [
        pltpu.make_async_copy(src, dst, loc_in.at[i])
        for i, (src, dst) in enumerate(zip((wg_ref, wu_ref, wd_ref), own))
    ]
    for copy in loads:
        copy.start()

    barrier = pltpu.get_barrier_semaphore()
    for step in range(1, NZ):
        pl.semaphore_signal(
            barrier, inc=1, device_id={"sp": dev(lax.rem(z + step, NZ), y, c)}, device_id_type=MESH
        )
    for target in (y_dev, c_dev):
        pl.semaphore_signal(barrier, inc=1, device_id={"sp": target}, device_id_type=MESH)
    pl.semaphore_wait(barrier, NZ + 1)

    def kv_slot(buf, shard):
        return buf.at[pl.ds(pl.multiple_of(shard * rows, rows), rows), :]

    def kv_copies(shard, first, kind, target):
        out = []
        for i, (src, buf) in enumerate(((k_ref, kbuf), (v_ref, vbuf))):
            dst = kv_slot(buf, shard)
            out.append(
                remote(src if first else dst, dst, kv_send.at[i, kind, shard], kv_recv.at[i, shard], target)
            )
        return out

    def own_part(a, part):
        if a < 2:
            return own[a].at[:, pl.ds(pl.multiple_of(part * units, 128), units)]
        return own[a].at[pl.ds(pl.multiple_of(part * units, 128), units), :]

    def slot(a, shard):
        if a < 2:
            return (gate_ref, up_ref)[a].at[pl.ds(pl.multiple_of(shard * depth, depth), depth), :]
        return down_ref.at[:, pl.ds(pl.multiple_of(shard * cols, cols), cols)]

    def w_copy(a, shard, kind, target, first=False, part=None):
        dst = slot(a, shard)
        src = own_part(a, half if part is None else part) if first else dst
        return remote(src, dst, w_send.at[a, kind, shard], w_recv.at[a, shard], target)

    for dz in range(1, NZ):
        @pl.when(z + dz < NZ)
        def _():
            for copy in kv_copies(sp, True, dz - 1, dev(z + dz, y, c)):
                copy.start()
    for kind, target in ((3, y_dev), (4, c_dev)):
        for copy in kv_copies(sp, True, kind, target):
            copy.start()

    for a in range(3):
        loads[a].wait()
        w_copy(a, sp, 0, dev(cross_in, y, c), True, 1 - half).start()
    for a in range(3):
        w_copy(a, sp, 1, m_dev, True).start()
        w_copy(a, sp, 3, c_dev, True).start()
    stores = [
        pltpu.make_async_copy(own_part(a, half), slot(a, sp), loc_out.at[a]) for a in range(3)
    ]
    for copy in stores:
        copy.start()

    lane_head = lax.broadcasted_iota(jnp.int32, (rows, width), 1) // HEAD_DIM
    q_all = q_ref[...].astype(jnp.float32) * HEAD_DIM ** (-0.5)
    for h in range(heads):
        qs[h] = jnp.where(lane_head == h, q_all, 0.0).astype(jnp.bfloat16)
    r_idx = lax.broadcasted_iota(jnp.int32, (rows, rows), 0)
    c_idx = lax.broadcasted_iota(jnp.int32, (rows, rows), 1)
    tri[...] = jnp.where(r_idx > c_idx, 1.0, 0.0).astype(jnp.bfloat16)
    acc[...] = jnp.zeros_like(acc)
    tail[...] = jnp.zeros_like(tail)

    def attend(kb, vb, masked):
        for h in range(heads):
            scores = lax.dot_general(
                qs[h], kb, (((1,), (1,)), ((), ())), preferred_element_type=jnp.float32
            ) - shift_ref[h]
            keep = -(jnp.maximum(scores, 0.0) + jnp.log(1.0 + jnp.exp(-jnp.abs(scores))))
            take = scores + keep
            if masked:
                keep = jnp.where(c_idx < r_idx, keep, 0.0)
            high = keep.astype(jnp.bfloat16)
            low = (keep - high.astype(jnp.float32)).astype(jnp.bfloat16)
            later = jnp.dot(high, tri[...], preferred_element_type=jnp.float32) + jnp.dot(
                low, tri[...], preferred_element_type=jnp.float32
            )
            before = tail[h]
            weights = jnp.exp(take + later + before[:, 0:1])
            if masked:
                weights = jnp.where(c_idx < r_idx, weights, 0.0)
            acc[h] += jnp.dot(weights.astype(jnp.bfloat16), vb, preferred_element_type=jnp.float32)
            tail[h] = before + (later[:, 0:1] + keep[:, 0:1])

    attend(k_ref[...], v_ref[...], True)

    for dz in range(1, NZ):
        @pl.when(z >= dz)
        def _():
            shard = dev(z - dz, y, c)
            for copy in kv_copies(shard, False, 3, y_dev):
                copy.wait_recv()
                copy.start()
            for copy in kv_copies(shard, False, 4, c_dev):
                copy.start()
    for a in range(3):
        w_copy(a, sp, 2, y_dev, True).start()
    for dz in range(NZ):
        @pl.when(z >= dz)
        def _():
            shard = dev(z - dz, 1 - y, c)
            for copy in kv_copies(shard, False, 4, c_dev):
                copy.wait_recv()
                copy.start()
    for dz in range(NZ):
        @pl.when(z >= dz)
        def _():
            for yy in (0, 1):
                for copy in kv_copies(dev(z - dz, yy, 1 - c), False, 4, c_dev):
                    copy.wait_recv()

    def blocks(first, last):
        def body(i, carry):
            shard = sp - i
            attend(kv_slot(kbuf, shard)[...], kv_slot(vbuf, shard)[...], False)
            return carry

        lax.fori_loop(jnp.minimum(first, sp + 1), jnp.minimum(last, sp + 1), body, 0)

    def arrived(zz, to_mate):
        shard = dev(zz, y, c)
        for a in range(3):
            w_copy(a, shard, 1, m_dev).wait_recv()
            if to_mate:
                w_copy(a, shard, 1, m_dev).start()
            w_copy(a, shard, 2, y_dev).start()
            w_copy(a, shard, 3, c_dev).start()

    blocks(1, 3)
    @pl.when(inner)
    def _():
        arrived(cross_in, True)
    blocks(3, 6)
    arrived(z_mate, False)
    blocks(6, 9)
    @pl.when(inner)
    def _():
        arrived(cross_out, True)
    blocks(9, NZ * NY * NC)

    total = jnp.zeros((rows, width), jnp.float32)
    for h in range(heads):
        total = jnp.where(lane_head == h, acc[h], total)
    att_ref[...] = total.astype(jnp.bfloat16)

    @pl.when(jnp.logical_not(inner))
    def _():
        arrived(cross_in, False)
        arrived(cross_out, False)
    for zz in (z, z_mate, cross_in, cross_out):
        for a in range(3):
            copy = w_copy(a, dev(zz, 1 - y, c), 3, c_dev)
            copy.wait_recv()
            copy.start()
    for zz in (z, z_mate, cross_in, cross_out):
        for yy in (y, 1 - y):
            for a in range(3):
                w_copy(a, dev(zz, yy, 1 - c), 3, c_dev).wait_recv()

    for copy in stores:
        copy.wait()
    for dz in range(1, NZ):
        @pl.when(z + dz < NZ)
        def _():
            for copy in kv_copies(sp, True, dz - 1, dev(z + dz, y, c)):
                copy.wait_send()
    for dz in range(NZ):
        @pl.when(z >= dz)
        def _():
            for copy in kv_copies(dev(z - dz, y, c), False, 3, y_dev):
                copy.wait_send()
            for yy in (y, 1 - y):
                for copy in kv_copies(dev(z - dz, yy, c), False, 4, c_dev):
                    copy.wait_send()
    for a in range(3):
        w_copy(a, sp, 0, m_dev).wait_send()
        w_copy(a, sp, 1, m_dev).wait_send()
        for zz in (z, z_mate, cross_in, cross_out):
            w_copy(a, dev(zz, y, c), 2, y_dev).wait_send()
            for yy in (y, 1 - y):
                w_copy(a, dev(zz, yy, c), 3, c_dev).wait_send()

    @pl.when(inner)
    def _():
        for zz in (cross_in, cross_out):
            for a in range(3):
                w_copy(a, dev(zz, y, c), 1, m_dev).wait_send()


def front(queries, keys, values, score_shift, w_gate, w_up, w_down):
    shards = lax.axis_size("sp")
    rows, width = queries.shape
    heads = width // HEAD_DIM
    depth, units = w_gate.shape[0], w_gate.shape[1] // 2
    cols = w_down.shape[1]
    vmem = pl.BlockSpec(memory_space=pltpu.VMEM)
    hbm = pl.BlockSpec(memory_space=pl.ANY)
    return pl.pallas_call(
        front_kernel,
        out_shape=(
            jax.ShapeDtypeStruct((rows, width), jnp.bfloat16),
            jax.ShapeDtypeStruct((shards * depth, units), jnp.bfloat16),
            jax.ShapeDtypeStruct((shards * depth, units), jnp.bfloat16),
            jax.ShapeDtypeStruct((units, shards * cols), jnp.bfloat16),
        ),
        in_specs=[vmem, vmem, vmem, pl.BlockSpec(memory_space=pltpu.SMEM), hbm, hbm, hbm],
        out_specs=(vmem, hbm, hbm, hbm),
        scratch_shapes=[
            pltpu.VMEM((shards * rows, width), jnp.bfloat16),
            pltpu.VMEM((shards * rows, width), jnp.bfloat16),
            pltpu.VMEM((heads, rows, width), jnp.bfloat16),
            pltpu.VMEM((heads, rows, width), jnp.float32),
            pltpu.VMEM((heads, rows, 128), jnp.float32),
            pltpu.VMEM((rows, rows), jnp.bfloat16),
            pltpu.VMEM(w_gate.shape, jnp.bfloat16),
            pltpu.VMEM(w_up.shape, jnp.bfloat16),
            pltpu.VMEM(w_down.shape, jnp.bfloat16),
            pltpu.SemaphoreType.DMA((2, 5, shards)),
            pltpu.SemaphoreType.DMA((2, shards)),
            pltpu.SemaphoreType.DMA((3, 4, shards)),
            pltpu.SemaphoreType.DMA((3, shards)),
            pltpu.SemaphoreType.DMA((3,)),
            pltpu.SemaphoreType.DMA((3,)),
        ],
        compiler_params=pltpu.CompilerParams(collective_id=0, has_side_effects=True),
        name="front",
    )(queries, keys, values, score_shift, w_gate, w_up, w_down)


def local(
    queries, keys, values, score_shift, resid, w_out, gain_mix, gain_pre,
    w_gate, w_up, conv_gate, conv_up, w_down, gain_post,
):
    attended, gate_w, up_w, down_w = front(
        queries, keys, values, score_shift, w_gate, w_up, w_down
    )
    shards = lax.axis_size("sp")
    hop = shards // 2
    sp = lax.axis_index("sp")
    half = sp // hop
    units = gate_w.shape[1]
    pairs = [(i, (i + hop) % shards) for i in range(shards)]
    head_rows = lax.all_to_all(attended, "tp", split_axis=0, concat_axis=1, tiled=True)
    mixed = jnp.dot(head_rows, w_out, preferred_element_type=jnp.float32).astype(jnp.bfloat16)
    middle = (resid.astype(jnp.float32) + gain_mix * rms_scale(mixed.astype(jnp.float32))).astype(
        jnp.bfloat16
    )
    normed = (gain_pre * rms_scale(middle.astype(jnp.float32))).astype(jnp.bfloat16)
    piece = lax.all_gather(normed, "tp", axis=0, tiled=True)
    other = lax.ppermute(piece, "sp", pairs)
    run = piece.shape[0]
    tokens = jnp.where(
        half == 0, jnp.concatenate([piece, other], 0), jnp.concatenate([other, piece], 0)
    )
    conv_g = lax.dynamic_slice_in_dim(conv_gate, half * units, units, 1)
    conv_u = lax.dynamic_slice_in_dim(conv_up, half * units, units, 1)
    gate_part = jnp.dot(tokens, gate_w, preferred_element_type=jnp.float32).astype(jnp.bfloat16)
    up_part = jnp.dot(tokens, up_w, preferred_element_type=jnp.float32).astype(jnp.bfloat16)
    last = KERNEL - 1
    edges = jnp.stack(
        [
            jnp.stack([part[run - last : run], part[2 * run - last :]])
            for part in (gate_part, up_part)
        ]
    )
    ring = [(i, i // hop * hop + (i + 1) % hop) for i in range(shards)]
    before = lax.ppermute(edges, "sp", ring)
    first = sp % hop == 0
    before = jnp.where(
        first, jnp.stack([jnp.zeros_like(before[:, 0]), before[:, 0]], axis=1), before
    )

    def convolve(part, edge, taps):
        out = []
        for r in range(2):
            ext = jnp.concatenate([edge[r], part[r * run : (r + 1) * run]], 0).astype(jnp.float32)
            total = taps[0] * ext[0:run]
            for tap in range(1, KERNEL):
                total = total + taps[tap] * ext[tap : tap + run]
            out.append(total)
        return jnp.concatenate(out, 0)

    hidden = (
        jax.nn.silu(convolve(gate_part, before[0], conv_g)) * convolve(up_part, before[1], conv_u)
    ).astype(jnp.bfloat16)
    partial = jnp.dot(hidden, down_w, preferred_element_type=jnp.float32).astype(jnp.bfloat16)
    away = lax.dynamic_slice_in_dim(partial, (1 - half) * run, run, 0)
    mine = lax.dynamic_slice_in_dim(partial, half * run, run, 0)
    back = lax.ppermute(away, "sp", pairs)
    both = (mine.astype(jnp.float32) + back.astype(jnp.float32)).astype(jnp.bfloat16)
    summed = lax.psum_scatter(both, "tp", scatter_dimension=0, tiled=True)
    return (middle.astype(jnp.float32) + gain_post * rms_scale(summed.astype(jnp.float32))).astype(
        jnp.bfloat16
    )


def solution(mesh):
    in_specs = (
        P("sp", "tp"),
        P("sp", "tp"),
        P("sp", "tp"),
        P("tp"),
        P(("sp", "tp"), None),
        P(),
        P(),
        P(),
        P("sp", "tp"),
        P("sp", "tp"),
        P(None, "tp"),
        P(None, "tp"),
        P("tp", "sp"),
        P(),
    )
    out_specs = P(("sp", "tp"), None)
    split = mesh.shape["sp"] == NZ * NY * NC and mesh.shape["tp"] == 2
    return jax.shard_map(local if split else generic_local, mesh=mesh, in_specs=in_specs, out_specs=out_specs, check_vma=False)
```

```python
import functools

import jax
import jax.numpy as jnp
from jax import lax
from jax.experimental import pallas as pl
from jax.experimental.pallas import tpu as pltpu
from jax.sharding import PartitionSpec as P

HEAD_DIM = 64
KERNEL = 3


def from_behind(x, axis, by):
    length = lax.axis_size(axis)
    pairs = [(i, i + by) for i in range(length) if 0 <= i + by < length]
    return lax.ppermute(x, axis, pairs)


def rms_scale(values_in):
    return values_in * lax.rsqrt(jnp.mean(values_in * values_in, axis=-1, keepdims=True) + 1e-06)


def collect_weights(w_gate, w_up, w_down):
    gate_whole, up_whole = (
        lax.all_gather(w_gate, "sp", axis=0, tiled=True),
        lax.all_gather(w_up, "sp", axis=0, tiled=True),
    )
    down_whole = lax.all_gather(w_down, "sp", axis=1, tiled=True)
    return (gate_whole, up_whole, down_whole)


def stick_attention(queries, key_whole, value_whole, score_shift):
    tok_rows = queries.shape[0]
    local_heads = queries.shape[1] // HEAD_DIM
    total = key_whole.shape[0]
    shards = total // tok_rows
    group = max(
        (
            factor
            for factor in range(1, shards + 1)
            if shards % factor == 0 and factor * tok_rows <= max(2048, tok_rows)
        )
    )
    span = group * tok_rows
    offset = lax.axis_index("sp") * tok_rows
    query_heads = queries.reshape(tok_rows, local_heads, HEAD_DIM)
    key_heads = key_whole.reshape(total, local_heads, HEAD_DIM)
    value_heads = value_whole.reshape(total, local_heads, HEAD_DIM)
    query_pos = offset + jnp.arange(tok_rows, dtype=jnp.int32)
    last_block = (offset + tok_rows - 1) // span

    def visit(turn, carry):
        accum, tail = carry
        block_start = (last_block - turn) * span
        key_block = lax.dynamic_slice_in_dim(key_heads, block_start, span, 0)
        value_block = lax.dynamic_slice_in_dim(value_heads, block_start, span, 0)
        scores = jnp.einsum(
            "qhd,khd->hqk", query_heads, key_block, preferred_element_type=jnp.float32
        )
        scores = scores * HEAD_DIM ** (-0.5) - score_shift[:, None, None]
        key_pos = block_start + jnp.arange(span, dtype=jnp.int32)
        causal = (key_pos[None, :] < query_pos[:, None])[None, :, :]
        log_keep = jnp.where(causal, -jax.nn.softplus(scores), 0.0)
        later = lax.cumsum(log_keep, axis=2, reverse=True) - log_keep
        weights = jnp.where(
            causal, jnp.exp(jax.nn.log_sigmoid(scores) + later + tail[:, :, None]), 0.0
        ).astype(jnp.bfloat16)
        accum = accum + jnp.einsum(
            "hqk,khd->hqd", weights, value_block, preferred_element_type=jnp.float32
        )
        return (accum, tail + jnp.sum(log_keep, axis=2))

    start_carry = (
        jnp.zeros((local_heads, tok_rows, HEAD_DIM), jnp.float32),
        jnp.zeros((local_heads, tok_rows), jnp.float32),
    )
    accum, _ = lax.fori_loop(0, last_block + 1, visit, start_carry)
    return accum.transpose(1, 0, 2).reshape(tok_rows, local_heads * HEAD_DIM).astype(jnp.bfloat16)


def generic_local(
    queries,
    keys,
    values,
    score_shift,
    resid,
    w_out,
    gain_mix,
    gain_pre,
    w_gate,
    w_up,
    conv_gate,
    conv_up,
    w_down,
    gain_post,
):
    gate_whole, up_whole, down_whole = collect_weights(w_gate, w_up, w_down)
    key_whole, value_whole = (
        lax.all_gather(keys, "sp", axis=0, tiled=True),
        lax.all_gather(values, "sp", axis=0, tiled=True),
    )
    attended = stick_attention(queries, key_whole, value_whole, score_shift)
    head_rows = lax.all_to_all(attended, "tp", split_axis=0, concat_axis=1, tiled=True)
    mixed = jnp.dot(head_rows, w_out, preferred_element_type=jnp.float32).astype(jnp.bfloat16)
    middle = (resid.astype(jnp.float32) + gain_mix * rms_scale(mixed.astype(jnp.float32))).astype(
        jnp.bfloat16
    )
    normed = (gain_pre * rms_scale(middle.astype(jnp.float32))).astype(jnp.bfloat16)
    piece = lax.all_gather(normed, "tp", axis=0, tiled=True)
    gate_part = jnp.dot(piece, gate_whole, preferred_element_type=jnp.float32).astype(jnp.bfloat16)
    up_part = jnp.dot(piece, up_whole, preferred_element_type=jnp.float32).astype(jnp.bfloat16)
    projected = jnp.concatenate([gate_part, up_part], axis=1)
    tok_rows = projected.shape[0]
    local_units = projected.shape[1] // 2
    edge = from_behind(projected[tok_rows - (KERNEL - 1) :], "sp", 1)
    extended = jnp.concatenate([edge, projected], axis=0).astype(jnp.float32)
    taps = jnp.concatenate([conv_gate, conv_up], axis=1)
    convolved = taps[0] * extended[0:tok_rows]
    for tap in range(1, KERNEL):
        convolved = convolved + taps[tap] * extended[tap : tap + tok_rows]
    hidden = (jax.nn.silu(convolved[:, :local_units]) * convolved[:, local_units:]).astype(
        jnp.bfloat16
    )
    summed = lax.psum_scatter(
        jnp.dot(hidden, down_whole, preferred_element_type=jnp.float32).astype(jnp.bfloat16),
        "tp",
        scatter_dimension=0,
        tiled=True,
    )
    return (middle.astype(jnp.float32) + gain_post * rms_scale(summed.astype(jnp.float32))).astype(
        jnp.bfloat16
    )


MESH = pl.DeviceIdType.MESH
NZ, NY, NC = 4, 2, 2


def front_kernel(
    q_ref, k_ref, v_ref, shift_ref, resid_ref, wo_ref, mix_ref, pre_ref, wg_ref, wu_ref, wd_ref,
    mid_ref, tok_ref, gate_ref, up_ref, down_ref,
    kbuf, vbuf, qs, acc, tail, tri, own_g, own_u, own_d, att, heads_in, mixed, normed,
    kv_send, kv_recv, w_send, w_recv, loc_in, loc_out, x_sem, t_send, t_recv,
):
    rows, width = q_ref.shape
    heads = width // HEAD_DIM
    depth = wg_ref.shape[0]
    units = gate_ref.shape[1]
    cols = wd_ref.shape[1]
    sp = lax.axis_index("sp")
    z, y, c = sp // (NY * NC), (sp // NC) % NY, sp % NC
    half = z // 2
    inner = (z == 1) | (z == 2)
    cross_in = 2 - half
    cross_out = 3 - 3 * half
    z_mate = z + 1 - 2 * lax.rem(z, 2)

    def dev(zz, yy, cc):
        return (zz * NY + yy) * NC + cc

    y_dev, c_dev, m_dev = dev(z, 1 - y, c), dev(z, y, 1 - c), dev(z_mate, y, c)

    def remote(src, dst, ssem, rsem, target):
        return pltpu.make_async_remote_copy(
            src_ref=src, dst_ref=dst, send_sem=ssem, recv_sem=rsem,
            device_id={"sp": target}, device_id_type=MESH,
        )

    own = (own_g, own_u, own_d)
    loads = [
        pltpu.make_async_copy(src, dst, loc_in.at[i])
        for i, (src, dst) in enumerate(zip((wg_ref, wu_ref, wd_ref), own))
    ]
    for copy in loads:
        copy.start()

    barrier = pltpu.get_barrier_semaphore()
    for step in range(1, NZ):
        pl.semaphore_signal(
            barrier, inc=1, device_id={"sp": dev(lax.rem(z + step, NZ), y, c)}, device_id_type=MESH
        )
    for target in (y_dev, c_dev):
        pl.semaphore_signal(barrier, inc=1, device_id={"sp": target}, device_id_type=MESH)
    tp = lax.axis_index("tp")
    pl.semaphore_signal(barrier, inc=1, device_id={"tp": 1 - tp}, device_id_type=MESH)
    pl.semaphore_wait(barrier, NZ + 2)

    def kv_slot(buf, shard):
        return buf.at[pl.ds(pl.multiple_of(shard * rows, rows), rows), :]

    def kv_copies(shard, first, kind, target):
        out = []
        for i, (src, buf) in enumerate(((k_ref, kbuf), (v_ref, vbuf))):
            dst = kv_slot(buf, shard)
            out.append(
                remote(src if first else dst, dst, kv_send.at[i, kind, shard], kv_recv.at[i, shard], target)
            )
        return out

    def own_part(a, part):
        if a < 2:
            return own[a].at[:, pl.ds(pl.multiple_of(part * units, 128), units)]
        return own[a].at[pl.ds(pl.multiple_of(part * units, 128), units), :]

    def slot(a, shard):
        if a < 2:
            return (gate_ref, up_ref)[a].at[pl.ds(pl.multiple_of(shard * depth, depth), depth), :]
        return down_ref.at[:, pl.ds(pl.multiple_of(shard * cols, cols), cols)]

    def w_copy(a, shard, kind, target, first=False, part=None):
        dst = slot(a, shard)
        src = own_part(a, half if part is None else part) if first else dst
        return remote(src, dst, w_send.at[a, kind, shard], w_recv.at[a, shard], target)

    for dz in range(1, NZ):
        @pl.when(z + dz < NZ)
        def _():
            for copy in kv_copies(sp, True, dz - 1, dev(z + dz, y, c)):
                copy.start()
    for kind, target in ((3, y_dev), (4, c_dev)):
        for copy in kv_copies(sp, True, kind, target):
            copy.start()

    for a in range(3):
        loads[a].wait()
        w_copy(a, sp, 0, dev(cross_in, y, c), True, 1 - half).start()
    for a in range(3):
        w_copy(a, sp, 1, m_dev, True).start()
        w_copy(a, sp, 3, c_dev, True).start()
    stores = [
        pltpu.make_async_copy(own_part(a, half), slot(a, sp), loc_out.at[a]) for a in range(3)
    ]
    for copy in stores:
        copy.start()

    lane_head = lax.broadcasted_iota(jnp.int32, (rows, width), 1) // HEAD_DIM
    q_all = q_ref[...].astype(jnp.float32) * HEAD_DIM ** (-0.5)
    for h in range(heads):
        qs[h] = jnp.where(lane_head == h, q_all, 0.0).astype(jnp.bfloat16)
    r_idx = lax.broadcasted_iota(jnp.int32, (rows, rows), 0)
    c_idx = lax.broadcasted_iota(jnp.int32, (rows, rows), 1)
    tri[...] = jnp.where(r_idx > c_idx, 1.0, 0.0).astype(jnp.bfloat16)
    acc[...] = jnp.zeros_like(acc)
    tail[...] = jnp.zeros_like(tail)

    def attend(kb, vb, masked):
        for h in range(heads):
            scores = lax.dot_general(
                qs[h], kb, (((1,), (1,)), ((), ())), preferred_element_type=jnp.float32
            ) - shift_ref[h]
            keep = -(jnp.maximum(scores, 0.0) + jnp.log(1.0 + jnp.exp(-jnp.abs(scores))))
            take = scores + keep
            if masked:
                keep = jnp.where(c_idx < r_idx, keep, 0.0)
            high = keep.astype(jnp.bfloat16)
            low = (keep - high.astype(jnp.float32)).astype(jnp.bfloat16)
            later = jnp.dot(high, tri[...], preferred_element_type=jnp.float32) + jnp.dot(
                low, tri[...], preferred_element_type=jnp.float32
            )
            before = tail[h]
            weights = jnp.exp(take + later + before[:, 0:1])
            if masked:
                weights = jnp.where(c_idx < r_idx, weights, 0.0)
            acc[h] += jnp.dot(weights.astype(jnp.bfloat16), vb, preferred_element_type=jnp.float32)
            tail[h] = before + (later[:, 0:1] + keep[:, 0:1])

    attend(k_ref[...], v_ref[...], True)

    for dz in range(1, NZ):
        @pl.when(z >= dz)
        def _():
            shard = dev(z - dz, y, c)
            for copy in kv_copies(shard, False, 3, y_dev):
                copy.wait_recv()
                copy.start()
            for copy in kv_copies(shard, False, 4, c_dev):
                copy.start()
        w_copy(dz - 1, sp, 2, y_dev, True).start()

    def plane(dz):
        for copy in kv_copies(dev(z - dz, 1 - y, c), False, 4, c_dev):
            copy.wait_recv()
            copy.start()
        for yy in (0, 1):
            for copy in kv_copies(dev(z - dz, yy, 1 - c), False, 4, c_dev):
                copy.wait_recv()
        in_plane = lax.rem(sp, NY * NC)
        if dz == 0:
            blocks(1, in_plane + 1)
        else:
            base = in_plane + (dz - 1) * NY * NC + 1
            blocks(base, base + NY * NC)

    def blocks(first, last):
        def body(i, carry):
            shard = sp - i
            attend(kv_slot(kbuf, shard)[...], kv_slot(vbuf, shard)[...], False)
            return carry

        lax.fori_loop(first, last, body, 0)

    def arrived(zz, to_mate):
        shard = dev(zz, y, c)
        for a in range(3):
            w_copy(a, shard, 1, m_dev).wait_recv()
            if to_mate:
                w_copy(a, shard, 1, m_dev).start()
            w_copy(a, shard, 2, y_dev).start()
            w_copy(a, shard, 3, c_dev).start()

    plane(0)
    @pl.when(inner)
    def _():
        arrived(cross_in, True)
    @pl.when(z >= 1)
    def _():
        plane(1)
    arrived(z_mate, False)
    @pl.when(z >= 2)
    def _():
        plane(2)
    @pl.when(inner)
    def _():
        arrived(cross_out, True)
    @pl.when(z >= 3)
    def _():
        plane(3)

    total = jnp.zeros((rows, width), jnp.float32)
    for h in range(heads):
        total = jnp.where(lane_head == h, acc[h], total)
    att[...] = total.astype(jnp.bfloat16)

    own_rows = rows // 2
    there = pl.ds(pl.multiple_of((1 - tp) * own_rows, own_rows), own_rows)
    here = pl.ds(pl.multiple_of(tp * own_rows, own_rows), own_rows)
    swap = pltpu.make_async_remote_copy(
        src_ref=att.at[there, :], dst_ref=heads_in, send_sem=x_sem.at[0], recv_sem=x_sem.at[1],
        device_id={"tp": 1 - tp}, device_id_type=MESH,
    )
    swap.start()

    @pl.when(jnp.logical_not(inner))
    def _():
        arrived(cross_in, False)

    out_rows = pl.ds(pl.multiple_of(tp * width, width), width)
    in_rows = pl.ds(pl.multiple_of((1 - tp) * width, width), width)
    wide = mixed.shape[1]
    step_cols = wide // 4
    for n in range(4):
        part = pl.ds(n * step_cols, step_cols)
        mixed[:, part] = jnp.dot(
            att[here, :], wo_ref[out_rows, part], preferred_element_type=jnp.float32
        )
    swap.wait_recv()
    for n in range(4):
        part = pl.ds(n * step_cols, step_cols)
        mixed[:, part] += jnp.dot(
            heads_in[...], wo_ref[in_rows, part], preferred_element_type=jnp.float32
        )

    @pl.loop(0, own_rows // 16)
    def _(i):
        part = pl.ds(pl.multiple_of(i * 16, 16), 16)
        value = mixed[part, :].astype(jnp.bfloat16).astype(jnp.float32)
        middle = (resid_ref[part, :].astype(jnp.float32) + mix_ref[...] * rms_scale(value)).astype(
            jnp.bfloat16
        )
        mid_ref[part, :] = middle
        normed[part, :] = (pre_ref[...] * rms_scale(middle.astype(jnp.float32))).astype(
            jnp.bfloat16
        )

    p_dev = dev(lax.rem(z + 2, NZ), y, c)

    def tok_slot(part, xx):
        first = (part * 2 + xx) * own_rows
        return tok_ref.at[pl.ds(pl.multiple_of(first, own_rows), own_rows), :]

    def tok_copy(src, part, xx, kind, target):
        return pltpu.make_async_remote_copy(
            src_ref=src, dst_ref=tok_slot(part, xx), send_sem=t_send.at[kind],
            recv_sem=t_recv.at[part, xx], device_id=target, device_id_type=MESH,
        )

    to_x = tok_copy(normed, half, tp, 0, {"tp": 1 - tp})
    to_p = tok_copy(normed, half, tp, 1, {"sp": p_dev})
    to_x.start()
    to_p.start()
    keep_own = pltpu.make_async_copy(normed, tok_slot(half, tp), x_sem.at[2])
    keep_own.start()
    relay = tok_copy(tok_slot(half, 1 - tp), half, 1 - tp, 2, {"sp": p_dev})
    relay.wait_recv()
    relay.start()

    @pl.when(jnp.logical_not(inner))
    def _():
        arrived(cross_out, False)
    for zz in (z, z_mate, cross_in, cross_out):
        for a in range(3):
            copy = w_copy(a, dev(zz, 1 - y, c), 3, c_dev)
            copy.wait_recv()
            copy.start()
    for zz in (z, z_mate, cross_in, cross_out):
        for yy in (y, 1 - y):
            for a in range(3):
                w_copy(a, dev(zz, yy, 1 - c), 3, c_dev).wait_recv()

    for xx in (tp, 1 - tp):
        tok_copy(normed, 1 - half, xx, 1, {"sp": p_dev}).wait_recv()

    for copy in (swap, to_x, to_p, relay):
        copy.wait_send()
    keep_own.wait()
    for copy in stores:
        copy.wait()
    for dz in range(1, NZ):
        @pl.when(z + dz < NZ)
        def _():
            for copy in kv_copies(sp, True, dz - 1, dev(z + dz, y, c)):
                copy.wait_send()
    for dz in range(NZ):
        @pl.when(z >= dz)
        def _():
            for copy in kv_copies(dev(z - dz, y, c), False, 3, y_dev):
                copy.wait_send()
            for yy in (y, 1 - y):
                for copy in kv_copies(dev(z - dz, yy, c), False, 4, c_dev):
                    copy.wait_send()
    for a in range(3):
        w_copy(a, sp, 0, m_dev).wait_send()
        w_copy(a, sp, 1, m_dev).wait_send()
        for zz in (z, z_mate, cross_in, cross_out):
            w_copy(a, dev(zz, y, c), 2, y_dev).wait_send()
            for yy in (y, 1 - y):
                w_copy(a, dev(zz, yy, c), 3, c_dev).wait_send()

    @pl.when(inner)
    def _():
        for zz in (cross_in, cross_out):
            for a in range(3):
                w_copy(a, dev(zz, y, c), 1, m_dev).wait_send()


def front(
    queries, keys, values, score_shift, resid, w_out, gain_mix, gain_pre, w_gate, w_up, w_down
):
    shards = lax.axis_size("sp")
    rows, width = queries.shape
    heads = width // HEAD_DIM
    depth, units = w_gate.shape[0], w_gate.shape[1] // 2
    cols = w_down.shape[1]
    vmem = pl.BlockSpec(memory_space=pltpu.VMEM)
    hbm = pl.BlockSpec(memory_space=pl.ANY)
    return pl.pallas_call(
        front_kernel,
        out_shape=(
            jax.ShapeDtypeStruct(resid.shape, jnp.bfloat16),
            jax.ShapeDtypeStruct((4 * resid.shape[0], resid.shape[1]), jnp.bfloat16),
            jax.ShapeDtypeStruct((shards * depth, units), jnp.bfloat16),
            jax.ShapeDtypeStruct((shards * depth, units), jnp.bfloat16),
            jax.ShapeDtypeStruct((units, shards * cols), jnp.bfloat16),
        ),
        in_specs=[vmem] * 3 + [pl.BlockSpec(memory_space=pltpu.SMEM)] + [vmem] * 4 + [hbm] * 3,
        out_specs=(vmem, hbm, hbm, hbm, hbm),
        scratch_shapes=[
            pltpu.VMEM((shards * rows, width), jnp.bfloat16),
            pltpu.VMEM((shards * rows, width), jnp.bfloat16),
            pltpu.VMEM((heads, rows, width), jnp.bfloat16),
            pltpu.VMEM((heads, rows, width), jnp.float32),
            pltpu.VMEM((heads, rows, 128), jnp.float32),
            pltpu.VMEM((rows, rows), jnp.bfloat16),
            pltpu.VMEM(w_gate.shape, jnp.bfloat16),
            pltpu.VMEM(w_up.shape, jnp.bfloat16),
            pltpu.VMEM(w_down.shape, jnp.bfloat16),
            pltpu.VMEM((rows, width), jnp.bfloat16),
            pltpu.VMEM((rows // 2, width), jnp.bfloat16),
            pltpu.VMEM(resid.shape, jnp.float32),
            pltpu.VMEM(resid.shape, jnp.bfloat16),
            pltpu.SemaphoreType.DMA((2, 5, shards)),
            pltpu.SemaphoreType.DMA((2, shards)),
            pltpu.SemaphoreType.DMA((3, 4, shards)),
            pltpu.SemaphoreType.DMA((3, shards)),
            pltpu.SemaphoreType.DMA((3,)),
            pltpu.SemaphoreType.DMA((3,)),
            pltpu.SemaphoreType.DMA((3,)),
            pltpu.SemaphoreType.DMA((3,)),
            pltpu.SemaphoreType.DMA((2, 2)),
        ],
        compiler_params=pltpu.CompilerParams(collective_id=0, has_side_effects=True),
        name="front",
    )(
        queries, keys, values, score_shift, resid, w_out, gain_mix[None], gain_pre[None],
        w_gate, w_up, w_down,
    )


def local(
    queries, keys, values, score_shift, resid, w_out, gain_mix, gain_pre,
    w_gate, w_up, conv_gate, conv_up, w_down, gain_post,
):
    middle, tokens, gate_w, up_w, down_w = front(
        queries, keys, values, score_shift, resid, w_out, gain_mix, gain_pre, w_gate, w_up, w_down
    )
    shards = lax.axis_size("sp")
    hop = shards // 2
    sp = lax.axis_index("sp")
    half = sp // hop
    units = gate_w.shape[1]
    pairs = [(i, (i + hop) % shards) for i in range(shards)]
    run = tokens.shape[0] // 2
    conv_g = lax.dynamic_slice_in_dim(conv_gate, half * units, units, 1)
    conv_u = lax.dynamic_slice_in_dim(conv_up, half * units, units, 1)
    gate_part = jnp.dot(tokens, gate_w, preferred_element_type=jnp.float32).astype(jnp.bfloat16)
    up_part = jnp.dot(tokens, up_w, preferred_element_type=jnp.float32).astype(jnp.bfloat16)
    last = KERNEL - 1
    edges = jnp.stack(
        [
            jnp.stack([part[run - last : run], part[2 * run - last :]])
            for part in (gate_part, up_part)
        ]
    )
    ring = [(i, i // hop * hop + (i + 1) % hop) for i in range(shards)]
    before = lax.ppermute(edges, "sp", ring)
    first = sp % hop == 0
    before = jnp.where(
        first, jnp.stack([jnp.zeros_like(before[:, 0]), before[:, 0]], axis=1), before
    )

    def convolve(part, edge, taps):
        out = []
        for r in range(2):
            ext = jnp.concatenate([edge[r], part[r * run : (r + 1) * run]], 0).astype(jnp.float32)
            total = taps[0] * ext[0:run]
            for tap in range(1, KERNEL):
                total = total + taps[tap] * ext[tap : tap + run]
            out.append(total)
        return jnp.concatenate(out, 0)

    hidden = (
        jax.nn.silu(convolve(gate_part, before[0], conv_g)) * convolve(up_part, before[1], conv_u)
    ).astype(jnp.bfloat16)
    partial = jnp.dot(hidden, down_w, preferred_element_type=jnp.float32).astype(jnp.bfloat16)
    away = lax.dynamic_slice_in_dim(partial, (1 - half) * run, run, 0)
    mine = lax.dynamic_slice_in_dim(partial, half * run, run, 0)
    back = lax.ppermute(away, "sp", pairs)
    both = (mine.astype(jnp.float32) + back.astype(jnp.float32)).astype(jnp.bfloat16)
    summed = lax.psum_scatter(both, "tp", scatter_dimension=0, tiled=True)
    return (middle.astype(jnp.float32) + gain_post * rms_scale(summed.astype(jnp.float32))).astype(
        jnp.bfloat16
    )


def solution(mesh):
    in_specs = (
        P("sp", "tp"),
        P("sp", "tp"),
        P("sp", "tp"),
        P("tp"),
        P(("sp", "tp"), None),
        P(),
        P(),
        P(),
        P("sp", "tp"),
        P("sp", "tp"),
        P(None, "tp"),
        P(None, "tp"),
        P("tp", "sp"),
        P(),
    )
    out_specs = P(("sp", "tp"), None)
    split = mesh.shape["sp"] == NZ * NY * NC and mesh.shape["tp"] == 2
    return jax.shard_map(local if split else generic_local, mesh=mesh, in_specs=in_specs, out_specs=out_specs, check_vma=False)
```

```python
import functools

import jax
import jax.numpy as jnp
from jax import lax
from jax.experimental import pallas as pl
from jax.experimental.pallas import tpu as pltpu
from jax.sharding import PartitionSpec as P

HEAD_DIM = 64
KERNEL = 3


def from_behind(x, axis, by):
    length = lax.axis_size(axis)
    pairs = [(i, i + by) for i in range(length) if 0 <= i + by < length]
    return lax.ppermute(x, axis, pairs)


def rms_scale(values_in):
    return values_in * lax.rsqrt(jnp.mean(values_in * values_in, axis=-1, keepdims=True) + 1e-06)


def collect_weights(w_gate, w_up, w_down):
    gate_whole, up_whole = (
        lax.all_gather(w_gate, "sp", axis=0, tiled=True),
        lax.all_gather(w_up, "sp", axis=0, tiled=True),
    )
    down_whole = lax.all_gather(w_down, "sp", axis=1, tiled=True)
    return (gate_whole, up_whole, down_whole)


def stick_attention(queries, key_whole, value_whole, score_shift):
    tok_rows = queries.shape[0]
    local_heads = queries.shape[1] // HEAD_DIM
    total = key_whole.shape[0]
    shards = total // tok_rows
    group = max(
        (
            factor
            for factor in range(1, shards + 1)
            if shards % factor == 0 and factor * tok_rows <= max(2048, tok_rows)
        )
    )
    span = group * tok_rows
    offset = lax.axis_index("sp") * tok_rows
    query_heads = queries.reshape(tok_rows, local_heads, HEAD_DIM)
    key_heads = key_whole.reshape(total, local_heads, HEAD_DIM)
    value_heads = value_whole.reshape(total, local_heads, HEAD_DIM)
    query_pos = offset + jnp.arange(tok_rows, dtype=jnp.int32)
    last_block = (offset + tok_rows - 1) // span

    def visit(turn, carry):
        accum, tail = carry
        block_start = (last_block - turn) * span
        key_block = lax.dynamic_slice_in_dim(key_heads, block_start, span, 0)
        value_block = lax.dynamic_slice_in_dim(value_heads, block_start, span, 0)
        scores = jnp.einsum(
            "qhd,khd->hqk", query_heads, key_block, preferred_element_type=jnp.float32
        )
        scores = scores * HEAD_DIM ** (-0.5) - score_shift[:, None, None]
        key_pos = block_start + jnp.arange(span, dtype=jnp.int32)
        causal = (key_pos[None, :] < query_pos[:, None])[None, :, :]
        log_keep = jnp.where(causal, -jax.nn.softplus(scores), 0.0)
        later = lax.cumsum(log_keep, axis=2, reverse=True) - log_keep
        weights = jnp.where(
            causal, jnp.exp(jax.nn.log_sigmoid(scores) + later + tail[:, :, None]), 0.0
        ).astype(jnp.bfloat16)
        accum = accum + jnp.einsum(
            "hqk,khd->hqd", weights, value_block, preferred_element_type=jnp.float32
        )
        return (accum, tail + jnp.sum(log_keep, axis=2))

    start_carry = (
        jnp.zeros((local_heads, tok_rows, HEAD_DIM), jnp.float32),
        jnp.zeros((local_heads, tok_rows), jnp.float32),
    )
    accum, _ = lax.fori_loop(0, last_block + 1, visit, start_carry)
    return accum.transpose(1, 0, 2).reshape(tok_rows, local_heads * HEAD_DIM).astype(jnp.bfloat16)


def generic_local(
    queries,
    keys,
    values,
    score_shift,
    resid,
    w_out,
    gain_mix,
    gain_pre,
    w_gate,
    w_up,
    conv_gate,
    conv_up,
    w_down,
    gain_post,
):
    gate_whole, up_whole, down_whole = collect_weights(w_gate, w_up, w_down)
    key_whole, value_whole = (
        lax.all_gather(keys, "sp", axis=0, tiled=True),
        lax.all_gather(values, "sp", axis=0, tiled=True),
    )
    attended = stick_attention(queries, key_whole, value_whole, score_shift)
    head_rows = lax.all_to_all(attended, "tp", split_axis=0, concat_axis=1, tiled=True)
    mixed = jnp.dot(head_rows, w_out, preferred_element_type=jnp.float32).astype(jnp.bfloat16)
    middle = (resid.astype(jnp.float32) + gain_mix * rms_scale(mixed.astype(jnp.float32))).astype(
        jnp.bfloat16
    )
    normed = (gain_pre * rms_scale(middle.astype(jnp.float32))).astype(jnp.bfloat16)
    piece = lax.all_gather(normed, "tp", axis=0, tiled=True)
    gate_part = jnp.dot(piece, gate_whole, preferred_element_type=jnp.float32).astype(jnp.bfloat16)
    up_part = jnp.dot(piece, up_whole, preferred_element_type=jnp.float32).astype(jnp.bfloat16)
    projected = jnp.concatenate([gate_part, up_part], axis=1)
    tok_rows = projected.shape[0]
    local_units = projected.shape[1] // 2
    edge = from_behind(projected[tok_rows - (KERNEL - 1) :], "sp", 1)
    extended = jnp.concatenate([edge, projected], axis=0).astype(jnp.float32)
    taps = jnp.concatenate([conv_gate, conv_up], axis=1)
    convolved = taps[0] * extended[0:tok_rows]
    for tap in range(1, KERNEL):
        convolved = convolved + taps[tap] * extended[tap : tap + tok_rows]
    hidden = (jax.nn.silu(convolved[:, :local_units]) * convolved[:, local_units:]).astype(
        jnp.bfloat16
    )
    summed = lax.psum_scatter(
        jnp.dot(hidden, down_whole, preferred_element_type=jnp.float32).astype(jnp.bfloat16),
        "tp",
        scatter_dimension=0,
        tiled=True,
    )
    return (middle.astype(jnp.float32) + gain_post * rms_scale(summed.astype(jnp.float32))).astype(
        jnp.bfloat16
    )


MESH = pl.DeviceIdType.MESH
NZ, NY, NC = 4, 2, 2


def front_kernel(
    q_ref, k_ref, v_ref, shift_ref, resid_ref, wo_ref, mix_ref, pre_ref, wg_ref, wu_ref, wd_ref,
    mid_ref, tok_ref, gate_ref, up_ref, down_ref,
    kbuf, vbuf, qs, acc, tail, tri, own_g, own_u, own_d, att, heads_in, mixed, normed,
    kv_send, kv_recv, w_send, w_recv, loc_in, loc_out, x_sem, t_send, t_recv,
):
    rows, width = q_ref.shape
    heads = width // HEAD_DIM
    depth = wg_ref.shape[0]
    units = gate_ref.shape[1]
    cols = wd_ref.shape[1]
    sp = lax.axis_index("sp")
    z, y, c = sp // (NY * NC), (sp // NC) % NY, sp % NC
    half = z // 2
    inner = (z == 1) | (z == 2)
    cross_in = 2 - half
    cross_out = 3 - 3 * half
    z_mate = z + 1 - 2 * lax.rem(z, 2)

    def dev(zz, yy, cc):
        return (zz * NY + yy) * NC + cc

    y_dev, c_dev, m_dev = dev(z, 1 - y, c), dev(z, y, 1 - c), dev(z_mate, y, c)

    def remote(src, dst, ssem, rsem, target):
        return pltpu.make_async_remote_copy(
            src_ref=src, dst_ref=dst, send_sem=ssem, recv_sem=rsem,
            device_id={"sp": target}, device_id_type=MESH,
        )

    own = (own_g, own_u, own_d)
    loads = [
        pltpu.make_async_copy(src, dst, loc_in.at[i])
        for i, (src, dst) in enumerate(zip((wg_ref, wu_ref, wd_ref), own))
    ]
    for copy in loads:
        copy.start()

    barrier = pltpu.get_barrier_semaphore()
    for step in range(1, NZ):
        pl.semaphore_signal(
            barrier, inc=1, device_id={"sp": dev(lax.rem(z + step, NZ), y, c)}, device_id_type=MESH
        )
    for target in (y_dev, c_dev):
        pl.semaphore_signal(barrier, inc=1, device_id={"sp": target}, device_id_type=MESH)
    tp = lax.axis_index("tp")
    pl.semaphore_signal(barrier, inc=1, device_id={"tp": 1 - tp}, device_id_type=MESH)
    pl.semaphore_wait(barrier, NZ + 2)

    def kv_slot(buf, shard):
        return buf.at[pl.ds(pl.multiple_of(shard * rows, rows), rows), :]

    def kv_copies(shard, first, kind, target):
        out = []
        for i, (src, buf) in enumerate(((k_ref, kbuf), (v_ref, vbuf))):
            dst = kv_slot(buf, shard)
            out.append(
                remote(src if first else dst, dst, kv_send.at[i, kind, shard], kv_recv.at[i, shard], target)
            )
        return out

    def own_part(a, part):
        if a < 2:
            return own[a].at[:, pl.ds(pl.multiple_of(part * units, 128), units)]
        return own[a].at[pl.ds(pl.multiple_of(part * units, 128), units), :]

    def slot(a, shard):
        if a < 2:
            return (gate_ref, up_ref)[a].at[pl.ds(pl.multiple_of(shard * depth, depth), depth), :]
        return down_ref.at[:, pl.ds(pl.multiple_of(shard * cols, cols), cols)]

    def w_copy(a, shard, kind, target, first=False, part=None):
        dst = slot(a, shard)
        src = own_part(a, half if part is None else part) if first else dst
        return remote(src, dst, w_send.at[a, kind, shard], w_recv.at[a, shard], target)

    for dz in range(1, NZ):
        @pl.when(z + dz < NZ)
        def _():
            for copy in kv_copies(sp, True, dz - 1, dev(z + dz, y, c)):
                copy.start()
    for kind, target in ((3, y_dev), (4, c_dev)):
        for copy in kv_copies(sp, True, kind, target):
            copy.start()

    for a in range(3):
        loads[a].wait()
        w_copy(a, sp, 0, dev(cross_in, y, c), True, 1 - half).start()
    for a in range(3):
        w_copy(a, sp, 1, m_dev, True).start()
        w_copy(a, sp, 3, c_dev, True).start()
    stores = [
        pltpu.make_async_copy(own_part(a, half), slot(a, sp), loc_out.at[a]) for a in range(3)
    ]
    for copy in stores:
        copy.start()

    lane_head = lax.broadcasted_iota(jnp.int32, (rows, width), 1) // HEAD_DIM
    q_all = q_ref[...].astype(jnp.float32) * HEAD_DIM ** (-0.5)
    for h in range(heads):
        qs[h] = jnp.where(lane_head == h, q_all, 0.0).astype(jnp.bfloat16)
    r_idx = lax.broadcasted_iota(jnp.int32, (rows, rows), 0)
    c_idx = lax.broadcasted_iota(jnp.int32, (rows, rows), 1)
    tri[...] = jnp.where(r_idx > c_idx, 1.0, 0.0).astype(jnp.bfloat16)
    acc[...] = jnp.zeros_like(acc)
    tail[...] = jnp.zeros_like(tail)

    def attend(kb, vb, masked):
        for h in range(heads):
            scores = lax.dot_general(
                qs[h], kb, (((1,), (1,)), ((), ())), preferred_element_type=jnp.float32
            ) - shift_ref[h]
            keep = -(jnp.maximum(scores, 0.0) + jnp.log(1.0 + jnp.exp(-jnp.abs(scores))))
            take = scores + keep
            if masked:
                keep = jnp.where(c_idx < r_idx, keep, 0.0)
            high = keep.astype(jnp.bfloat16)
            low = (keep - high.astype(jnp.float32)).astype(jnp.bfloat16)
            later = jnp.dot(high, tri[...], preferred_element_type=jnp.float32) + jnp.dot(
                low, tri[...], preferred_element_type=jnp.float32
            )
            before = tail[h]
            weights = jnp.exp(take + later + before[:, 0:1])
            if masked:
                weights = jnp.where(c_idx < r_idx, weights, 0.0)
            acc[h] += jnp.dot(weights.astype(jnp.bfloat16), vb, preferred_element_type=jnp.float32)
            tail[h] = before + (later[:, 0:1] + keep[:, 0:1])

    attend(k_ref[...], v_ref[...], True)

    for dz in range(1, NZ):
        @pl.when(z >= dz)
        def _():
            shard = dev(z - dz, y, c)
            for copy in kv_copies(shard, False, 3, y_dev):
                copy.wait_recv()
                copy.start()
            for copy in kv_copies(shard, False, 4, c_dev):
                copy.start()
        w_copy(dz - 1, sp, 2, y_dev, True).start()

    def plane(dz):
        for copy in kv_copies(dev(z - dz, 1 - y, c), False, 4, c_dev):
            copy.wait_recv()
            copy.start()
        for yy in (0, 1):
            for copy in kv_copies(dev(z - dz, yy, 1 - c), False, 4, c_dev):
                copy.wait_recv()
        in_plane = lax.rem(sp, NY * NC)
        if dz == 0:
            blocks(1, in_plane + 1)
        else:
            base = in_plane + (dz - 1) * NY * NC + 1
            blocks(base, base + NY * NC)

    def blocks(first, last):
        def body(i, carry):
            shard = sp - i
            attend(kv_slot(kbuf, shard)[...], kv_slot(vbuf, shard)[...], False)
            return carry

        lax.fori_loop(first, last, body, 0)

    def arrived(zz, to_mate):
        shard = dev(zz, y, c)
        for a in range(3):
            w_copy(a, shard, 1, m_dev).wait_recv()
            if to_mate:
                w_copy(a, shard, 1, m_dev).start()
            w_copy(a, shard, 2, y_dev).start()
            w_copy(a, shard, 3, c_dev).start()

    plane(0)
    @pl.when(inner)
    def _():
        arrived(cross_in, True)
    @pl.when(z >= 1)
    def _():
        plane(1)
    arrived(z_mate, False)
    @pl.when(z >= 2)
    def _():
        plane(2)
    @pl.when(inner)
    def _():
        arrived(cross_out, True)
    @pl.when(z >= 3)
    def _():
        plane(3)

    total = jnp.zeros((rows, width), jnp.float32)
    for h in range(heads):
        total = jnp.where(lane_head == h, acc[h], total)
    att[...] = total.astype(jnp.bfloat16)

    own_rows = rows // 2
    there = pl.ds(pl.multiple_of((1 - tp) * own_rows, own_rows), own_rows)
    here = pl.ds(pl.multiple_of(tp * own_rows, own_rows), own_rows)
    swap = pltpu.make_async_remote_copy(
        src_ref=att.at[there, :], dst_ref=heads_in, send_sem=x_sem.at[0], recv_sem=x_sem.at[1],
        device_id={"tp": 1 - tp}, device_id_type=MESH,
    )
    swap.start()

    @pl.when(jnp.logical_not(inner))
    def _():
        arrived(cross_in, False)

    out_rows = pl.ds(pl.multiple_of(tp * width, width), width)
    in_rows = pl.ds(pl.multiple_of((1 - tp) * width, width), width)
    wide = mixed.shape[1]
    step_cols = wide // 4
    for n in range(4):
        part = pl.ds(n * step_cols, step_cols)
        mixed[:, part] = jnp.dot(
            att[here, :], wo_ref[out_rows, part], preferred_element_type=jnp.float32
        )
    swap.wait_recv()
    for n in range(4):
        part = pl.ds(n * step_cols, step_cols)
        mixed[:, part] += jnp.dot(
            heads_in[...], wo_ref[in_rows, part], preferred_element_type=jnp.float32
        )

    @pl.loop(0, own_rows // 16)
    def _(i):
        part = pl.ds(pl.multiple_of(i * 16, 16), 16)
        value = mixed[part, :].astype(jnp.bfloat16).astype(jnp.float32)
        middle = (resid_ref[part, :].astype(jnp.float32) + mix_ref[...] * rms_scale(value)).astype(
            jnp.bfloat16
        )
        mid_ref[part, :] = middle
        normed[part, :] = (pre_ref[...] * rms_scale(middle.astype(jnp.float32))).astype(
            jnp.bfloat16
        )

    p_dev = dev(lax.rem(z + 2, NZ), y, c)

    def tok_slot(part, xx):
        first = (part * 2 + xx) * own_rows
        return tok_ref.at[pl.ds(pl.multiple_of(first, own_rows), own_rows), :]

    def tok_copy(src, part, xx, kind, target):
        return pltpu.make_async_remote_copy(
            src_ref=src, dst_ref=tok_slot(part, xx), send_sem=t_send.at[kind],
            recv_sem=t_recv.at[part, xx], device_id=target, device_id_type=MESH,
        )

    to_x = tok_copy(normed, half, tp, 0, {"tp": 1 - tp})
    to_p = tok_copy(normed, half, tp, 1, {"sp": p_dev})
    to_x.start()
    to_p.start()
    keep_own = pltpu.make_async_copy(normed, tok_slot(half, tp), x_sem.at[2])
    keep_own.start()
    relay = tok_copy(tok_slot(half, 1 - tp), half, 1 - tp, 2, {"sp": p_dev})
    relay.wait_recv()
    relay.start()

    @pl.when(jnp.logical_not(inner))
    def _():
        arrived(cross_out, False)
    for zz in (z, z_mate, cross_in, cross_out):
        for a in range(3):
            copy = w_copy(a, dev(zz, 1 - y, c), 3, c_dev)
            copy.wait_recv()
            copy.start()
    for zz in (z, z_mate, cross_in, cross_out):
        for yy in (y, 1 - y):
            for a in range(3):
                w_copy(a, dev(zz, yy, 1 - c), 3, c_dev).wait_recv()

    for xx in (tp, 1 - tp):
        tok_copy(normed, 1 - half, xx, 1, {"sp": p_dev}).wait_recv()

    for copy in (swap, to_x, to_p, relay):
        copy.wait_send()
    keep_own.wait()
    for copy in stores:
        copy.wait()
    for dz in range(1, NZ):
        @pl.when(z + dz < NZ)
        def _():
            for copy in kv_copies(sp, True, dz - 1, dev(z + dz, y, c)):
                copy.wait_send()
    for dz in range(NZ):
        @pl.when(z >= dz)
        def _():
            for copy in kv_copies(dev(z - dz, y, c), False, 3, y_dev):
                copy.wait_send()
            for yy in (y, 1 - y):
                for copy in kv_copies(dev(z - dz, yy, c), False, 4, c_dev):
                    copy.wait_send()
    for a in range(3):
        w_copy(a, sp, 0, m_dev).wait_send()
        w_copy(a, sp, 1, m_dev).wait_send()
        for zz in (z, z_mate, cross_in, cross_out):
            w_copy(a, dev(zz, y, c), 2, y_dev).wait_send()
            for yy in (y, 1 - y):
                w_copy(a, dev(zz, yy, c), 3, c_dev).wait_send()

    @pl.when(inner)
    def _():
        for zz in (cross_in, cross_out):
            for a in range(3):
                w_copy(a, dev(zz, y, c), 1, m_dev).wait_send()


def front(
    queries, keys, values, score_shift, resid, w_out, gain_mix, gain_pre, w_gate, w_up, w_down
):
    shards = lax.axis_size("sp")
    rows, width = queries.shape
    heads = width // HEAD_DIM
    depth, units = w_gate.shape[0], w_gate.shape[1] // 2
    cols = w_down.shape[1]
    vmem = pl.BlockSpec(memory_space=pltpu.VMEM)
    hbm = pl.BlockSpec(memory_space=pl.ANY)
    return pl.pallas_call(
        front_kernel,
        out_shape=(
            jax.ShapeDtypeStruct(resid.shape, jnp.bfloat16),
            jax.ShapeDtypeStruct((4 * resid.shape[0], resid.shape[1]), jnp.bfloat16),
            jax.ShapeDtypeStruct((shards * depth, units), jnp.bfloat16),
            jax.ShapeDtypeStruct((shards * depth, units), jnp.bfloat16),
            jax.ShapeDtypeStruct((units, shards * cols), jnp.bfloat16),
        ),
        in_specs=[vmem] * 3 + [pl.BlockSpec(memory_space=pltpu.SMEM)] + [vmem] * 4 + [hbm] * 3,
        out_specs=(vmem, hbm, hbm, hbm, hbm),
        scratch_shapes=[
            pltpu.VMEM((shards * rows, width), jnp.bfloat16),
            pltpu.VMEM((shards * rows, width), jnp.bfloat16),
            pltpu.VMEM((heads, rows, width), jnp.bfloat16),
            pltpu.VMEM((heads, rows, width), jnp.float32),
            pltpu.VMEM((heads, rows, 128), jnp.float32),
            pltpu.VMEM((rows, rows), jnp.bfloat16),
            pltpu.VMEM(w_gate.shape, jnp.bfloat16),
            pltpu.VMEM(w_up.shape, jnp.bfloat16),
            pltpu.VMEM(w_down.shape, jnp.bfloat16),
            pltpu.VMEM((rows, width), jnp.bfloat16),
            pltpu.VMEM((rows // 2, width), jnp.bfloat16),
            pltpu.VMEM(resid.shape, jnp.float32),
            pltpu.VMEM(resid.shape, jnp.bfloat16),
            pltpu.SemaphoreType.DMA((2, 5, shards)),
            pltpu.SemaphoreType.DMA((2, shards)),
            pltpu.SemaphoreType.DMA((3, 4, shards)),
            pltpu.SemaphoreType.DMA((3, shards)),
            pltpu.SemaphoreType.DMA((3,)),
            pltpu.SemaphoreType.DMA((3,)),
            pltpu.SemaphoreType.DMA((3,)),
            pltpu.SemaphoreType.DMA((3,)),
            pltpu.SemaphoreType.DMA((2, 2)),
        ],
        compiler_params=pltpu.CompilerParams(collective_id=0, has_side_effects=True),
        name="front",
    )(
        queries, keys, values, score_shift, resid, w_out, gain_mix[None], gain_pre[None],
        w_gate, w_up, w_down,
    )


def back_kernel(
    hid_ref, down_ref, mid_ref, post_ref, out_ref,
    own, out_x, in_x, out_z, in_z, x_send, x_recv, z_send, z_recv,
):
    rows, wide = mid_ref.shape
    parts = x_recv.shape[1]
    step_cols = wide // parts
    shards = NZ * NY * NC
    hop = shards // 2
    sp, tp = lax.axis_index("sp"), lax.axis_index("tp")
    half = sp // hop
    pair = lax.rem(sp + hop, shards)

    barrier = pltpu.get_barrier_semaphore()
    pl.semaphore_signal(barrier, inc=1, device_id={"tp": 1 - tp}, device_id_type=MESH)
    pl.semaphore_signal(barrier, inc=1, device_id={"sp": pair}, device_id_type=MESH)
    pl.semaphore_wait(barrier, 2)

    def block(part, xx):
        return hid_ref[pl.ds(pl.multiple_of((part * 2 + xx) * rows, rows), rows), :]

    def along_x(i, n):
        chunk = pl.ds(n * step_cols, step_cols)
        return pltpu.make_async_remote_copy(
            src_ref=out_x.at[i, :, chunk], dst_ref=in_x.at[i, :, chunk],
            send_sem=x_send.at[i, n], recv_sem=x_recv.at[i, n],
            device_id={"tp": 1 - tp}, device_id_type=MESH,
        )

    def along_z(n):
        chunk = pl.ds(n * step_cols, step_cols)
        return pltpu.make_async_remote_copy(
            src_ref=out_z.at[:, chunk], dst_ref=in_z.at[:, chunk],
            send_sem=z_send.at[n], recv_sem=z_recv.at[n],
            device_id={"sp": pair}, device_id_type=MESH,
        )

    def product(lhs, n):
        return jnp.dot(
            lhs, down_ref[:, n * step_cols : (n + 1) * step_cols],
            preferred_element_type=jnp.float32,
        ).astype(jnp.bfloat16)

    theirs = jnp.concatenate([block(1 - half, 1 - tp), block(half, 1 - tp)], axis=0)
    for n in range(parts):
        value = product(theirs, n)
        out_x[0, :, n * step_cols : (n + 1) * step_cols] = value[:rows]
        out_x[1, :, n * step_cols : (n + 1) * step_cols] = value[rows:]
        along_x(0, n).start()
    for n in range(parts):
        along_x(1, n).start()
    mine = jnp.concatenate([block(1 - half, tp), block(half, tp)], axis=0)
    for n in range(parts):
        value = product(mine, n)
        own[0, :, n * step_cols : (n + 1) * step_cols] = value[:rows]
        own[1, :, n * step_cols : (n + 1) * step_cols] = value[rows:]
    for n in range(parts):
        chunk = pl.ds(n * step_cols, step_cols)
        along_x(0, n).wait_recv()
        out_z[:, chunk] = (
            own[0, :, chunk].astype(jnp.float32) + in_x[0, :, chunk].astype(jnp.float32)
        ).astype(jnp.bfloat16)
        along_z(n).start()
    for n in range(parts):
        along_x(1, n).wait_recv()
    for n in range(parts):
        along_z(n).wait_recv()

    @pl.loop(0, rows // 16)
    def _(i):
        part = pl.ds(pl.multiple_of(i * 16, 16), 16)
        total = own[1, part, :].astype(jnp.float32) + in_x[1, part, :].astype(jnp.float32)
        total = (total + in_z[part, :].astype(jnp.float32)).astype(jnp.bfloat16)
        out_ref[part, :] = (
            mid_ref[part, :].astype(jnp.float32)
            + post_ref[...] * rms_scale(total.astype(jnp.float32))
        ).astype(jnp.bfloat16)

    for n in range(parts):
        along_x(0, n).wait_send()
        along_x(1, n).wait_send()
        along_z(n).wait_send()


def back(hidden, down_w, middle, gain_post):
    vmem = pl.BlockSpec(memory_space=pltpu.VMEM)
    parts = 4
    pair = pltpu.VMEM((2,) + middle.shape, jnp.bfloat16)
    one = pltpu.VMEM(middle.shape, jnp.bfloat16)
    return pl.pallas_call(
        back_kernel,
        out_shape=jax.ShapeDtypeStruct(middle.shape, jnp.bfloat16),
        in_specs=[vmem] * 4,
        out_specs=vmem,
        scratch_shapes=[
            pair, pair, pair, one, one,
            pltpu.SemaphoreType.DMA((2, parts)),
            pltpu.SemaphoreType.DMA((2, parts)),
            pltpu.SemaphoreType.DMA((parts,)),
            pltpu.SemaphoreType.DMA((parts,)),
        ],
        compiler_params=pltpu.CompilerParams(collective_id=1, has_side_effects=True),
        name="back",
    )(hidden, down_w, middle, gain_post[None])


def local(
    queries, keys, values, score_shift, resid, w_out, gain_mix, gain_pre,
    w_gate, w_up, conv_gate, conv_up, w_down, gain_post,
):
    middle, tokens, gate_w, up_w, down_w = front(
        queries, keys, values, score_shift, resid, w_out, gain_mix, gain_pre, w_gate, w_up, w_down
    )
    shards = lax.axis_size("sp")
    hop = shards // 2
    sp = lax.axis_index("sp")
    half = sp // hop
    units = gate_w.shape[1]
    run = tokens.shape[0] // 2
    conv_g = lax.dynamic_slice_in_dim(conv_gate, half * units, units, 1)
    conv_u = lax.dynamic_slice_in_dim(conv_up, half * units, units, 1)
    gate_part = jnp.dot(tokens, gate_w, preferred_element_type=jnp.float32).astype(jnp.bfloat16)
    up_part = jnp.dot(tokens, up_w, preferred_element_type=jnp.float32).astype(jnp.bfloat16)
    last = KERNEL - 1
    edges = jnp.stack(
        [
            jnp.stack([part[run - last : run], part[2 * run - last :]])
            for part in (gate_part, up_part)
        ]
    )
    ring = [(i, i // hop * hop + (i + 1) % hop) for i in range(shards)]
    before = lax.ppermute(edges, "sp", ring)
    first = sp % hop == 0
    before = jnp.where(
        first, jnp.stack([jnp.zeros_like(before[:, 0]), before[:, 0]], axis=1), before
    )

    def convolve(part, edge, taps):
        out = []
        for r in range(2):
            ext = jnp.concatenate([edge[r], part[r * run : (r + 1) * run]], 0).astype(jnp.float32)
            total = taps[0] * ext[0:run]
            for tap in range(1, KERNEL):
                total = total + taps[tap] * ext[tap : tap + run]
            out.append(total)
        return jnp.concatenate(out, 0)

    hidden = (
        jax.nn.silu(convolve(gate_part, before[0], conv_g)) * convolve(up_part, before[1], conv_u)
    ).astype(jnp.bfloat16)
    return back(hidden, down_w, middle, gain_post)


def solution(mesh):
    in_specs = (
        P("sp", "tp"),
        P("sp", "tp"),
        P("sp", "tp"),
        P("tp"),
        P(("sp", "tp"), None),
        P(),
        P(),
        P(),
        P("sp", "tp"),
        P("sp", "tp"),
        P(None, "tp"),
        P(None, "tp"),
        P("tp", "sp"),
        P(),
    )
    out_specs = P(("sp", "tp"), None)
    split = mesh.shape["sp"] == NZ * NY * NC and mesh.shape["tp"] == 2
    return jax.shard_map(local if split else generic_local, mesh=mesh, in_specs=in_specs, out_specs=out_specs, check_vma=False)
```

```python
import functools

import jax
import jax.numpy as jnp
from jax import lax
from jax.experimental import pallas as pl
from jax.experimental.pallas import tpu as pltpu
from jax.sharding import PartitionSpec as P

HEAD_DIM = 64
KERNEL = 3


def from_behind(x, axis, by):
    length = lax.axis_size(axis)
    pairs = [(i, i + by) for i in range(length) if 0 <= i + by < length]
    return lax.ppermute(x, axis, pairs)


def rms_scale(values_in):
    return values_in * lax.rsqrt(jnp.mean(values_in * values_in, axis=-1, keepdims=True) + 1e-06)


def collect_weights(w_gate, w_up, w_down):
    gate_whole, up_whole = (
        lax.all_gather(w_gate, "sp", axis=0, tiled=True),
        lax.all_gather(w_up, "sp", axis=0, tiled=True),
    )
    down_whole = lax.all_gather(w_down, "sp", axis=1, tiled=True)
    return (gate_whole, up_whole, down_whole)


def stick_attention(queries, key_whole, value_whole, score_shift):
    tok_rows = queries.shape[0]
    local_heads = queries.shape[1] // HEAD_DIM
    total = key_whole.shape[0]
    shards = total // tok_rows
    group = max(
        (
            factor
            for factor in range(1, shards + 1)
            if shards % factor == 0 and factor * tok_rows <= max(2048, tok_rows)
        )
    )
    span = group * tok_rows
    offset = lax.axis_index("sp") * tok_rows
    query_heads = queries.reshape(tok_rows, local_heads, HEAD_DIM)
    key_heads = key_whole.reshape(total, local_heads, HEAD_DIM)
    value_heads = value_whole.reshape(total, local_heads, HEAD_DIM)
    query_pos = offset + jnp.arange(tok_rows, dtype=jnp.int32)
    last_block = (offset + tok_rows - 1) // span

    def visit(turn, carry):
        accum, tail = carry
        block_start = (last_block - turn) * span
        key_block = lax.dynamic_slice_in_dim(key_heads, block_start, span, 0)
        value_block = lax.dynamic_slice_in_dim(value_heads, block_start, span, 0)
        scores = jnp.einsum(
            "qhd,khd->hqk", query_heads, key_block, preferred_element_type=jnp.float32
        )
        scores = scores * HEAD_DIM ** (-0.5) - score_shift[:, None, None]
        key_pos = block_start + jnp.arange(span, dtype=jnp.int32)
        causal = (key_pos[None, :] < query_pos[:, None])[None, :, :]
        log_keep = jnp.where(causal, -jax.nn.softplus(scores), 0.0)
        later = lax.cumsum(log_keep, axis=2, reverse=True) - log_keep
        weights = jnp.where(
            causal, jnp.exp(jax.nn.log_sigmoid(scores) + later + tail[:, :, None]), 0.0
        ).astype(jnp.bfloat16)
        accum = accum + jnp.einsum(
            "hqk,khd->hqd", weights, value_block, preferred_element_type=jnp.float32
        )
        return (accum, tail + jnp.sum(log_keep, axis=2))

    start_carry = (
        jnp.zeros((local_heads, tok_rows, HEAD_DIM), jnp.float32),
        jnp.zeros((local_heads, tok_rows), jnp.float32),
    )
    accum, _ = lax.fori_loop(0, last_block + 1, visit, start_carry)
    return accum.transpose(1, 0, 2).reshape(tok_rows, local_heads * HEAD_DIM).astype(jnp.bfloat16)


def generic_local(
    queries,
    keys,
    values,
    score_shift,
    resid,
    w_out,
    gain_mix,
    gain_pre,
    w_gate,
    w_up,
    conv_gate,
    conv_up,
    w_down,
    gain_post,
):
    gate_whole, up_whole, down_whole = collect_weights(w_gate, w_up, w_down)
    key_whole, value_whole = (
        lax.all_gather(keys, "sp", axis=0, tiled=True),
        lax.all_gather(values, "sp", axis=0, tiled=True),
    )
    attended = stick_attention(queries, key_whole, value_whole, score_shift)
    head_rows = lax.all_to_all(attended, "tp", split_axis=0, concat_axis=1, tiled=True)
    mixed = jnp.dot(head_rows, w_out, preferred_element_type=jnp.float32).astype(jnp.bfloat16)
    middle = (resid.astype(jnp.float32) + gain_mix * rms_scale(mixed.astype(jnp.float32))).astype(
        jnp.bfloat16
    )
    normed = (gain_pre * rms_scale(middle.astype(jnp.float32))).astype(jnp.bfloat16)
    piece = lax.all_gather(normed, "tp", axis=0, tiled=True)
    gate_part = jnp.dot(piece, gate_whole, preferred_element_type=jnp.float32).astype(jnp.bfloat16)
    up_part = jnp.dot(piece, up_whole, preferred_element_type=jnp.float32).astype(jnp.bfloat16)
    projected = jnp.concatenate([gate_part, up_part], axis=1)
    tok_rows = projected.shape[0]
    local_units = projected.shape[1] // 2
    edge = from_behind(projected[tok_rows - (KERNEL - 1) :], "sp", 1)
    extended = jnp.concatenate([edge, projected], axis=0).astype(jnp.float32)
    taps = jnp.concatenate([conv_gate, conv_up], axis=1)
    convolved = taps[0] * extended[0:tok_rows]
    for tap in range(1, KERNEL):
        convolved = convolved + taps[tap] * extended[tap : tap + tok_rows]
    hidden = (jax.nn.silu(convolved[:, :local_units]) * convolved[:, local_units:]).astype(
        jnp.bfloat16
    )
    summed = lax.psum_scatter(
        jnp.dot(hidden, down_whole, preferred_element_type=jnp.float32).astype(jnp.bfloat16),
        "tp",
        scatter_dimension=0,
        tiled=True,
    )
    return (middle.astype(jnp.float32) + gain_post * rms_scale(summed.astype(jnp.float32))).astype(
        jnp.bfloat16
    )


MESH = pl.DeviceIdType.MESH
NZ, NY, NC = 4, 2, 2


def front_kernel(
    q_ref, k_ref, v_ref, shift_ref, resid_ref, wo_ref, mix_ref, pre_ref, wg_ref, wu_ref, wd_ref,
    mid_ref, tok_ref, gate_ref, up_ref, down_ref,
    kbuf, vbuf, qs, acc, tail, tri, own_g, own_u, own_d, att, heads_in, mixed, normed,
    kv_send, kv_recv, w_send, w_recv, loc_in, loc_out, x_sem, t_send, t_recv,
):
    rows, width = q_ref.shape
    heads = width // HEAD_DIM
    depth = wg_ref.shape[0]
    units = gate_ref.shape[1]
    cols = wd_ref.shape[1]
    sp = lax.axis_index("sp")
    z, y, c = sp // (NY * NC), (sp // NC) % NY, sp % NC
    half = z // 2
    inner = (z == 1) | (z == 2)
    cross_in = 2 - half
    cross_out = 3 - 3 * half
    z_mate = z + 1 - 2 * lax.rem(z, 2)

    def dev(zz, yy, cc):
        return (zz * NY + yy) * NC + cc

    y_dev, c_dev, m_dev = dev(z, 1 - y, c), dev(z, y, 1 - c), dev(z_mate, y, c)

    def remote(src, dst, ssem, rsem, target):
        return pltpu.make_async_remote_copy(
            src_ref=src, dst_ref=dst, send_sem=ssem, recv_sem=rsem,
            device_id={"sp": target}, device_id_type=MESH,
        )

    own = (own_g, own_u, own_d)
    loads = [
        pltpu.make_async_copy(src, dst, loc_in.at[i])
        for i, (src, dst) in enumerate(zip((wg_ref, wu_ref, wd_ref), own))
    ]
    for copy in loads:
        copy.start()

    barrier = pltpu.get_barrier_semaphore()
    for step in range(1, NZ):
        pl.semaphore_signal(
            barrier, inc=1, device_id={"sp": dev(lax.rem(z + step, NZ), y, c)}, device_id_type=MESH
        )
    for target in (y_dev, c_dev):
        pl.semaphore_signal(barrier, inc=1, device_id={"sp": target}, device_id_type=MESH)
    tp = lax.axis_index("tp")
    pl.semaphore_signal(barrier, inc=1, device_id={"tp": 1 - tp}, device_id_type=MESH)
    pl.semaphore_wait(barrier, NZ + 2)

    def kv_slot(buf, shard):
        return buf.at[pl.ds(pl.multiple_of(shard * rows, rows), rows), :]

    def kv_copies(shard, first, kind, target):
        out = []
        for i, (src, buf) in enumerate(((k_ref, kbuf), (v_ref, vbuf))):
            dst = kv_slot(buf, shard)
            out.append(
                remote(src if first else dst, dst, kv_send.at[i, kind, shard], kv_recv.at[i, shard], target)
            )
        return out

    def own_part(a, part):
        if a < 2:
            return own[a].at[:, pl.ds(pl.multiple_of(part * units, 128), units)]
        return own[a].at[pl.ds(pl.multiple_of(part * units, 128), units), :]

    def slot(a, shard):
        if a < 2:
            return (gate_ref, up_ref)[a].at[pl.ds(pl.multiple_of(shard * depth, depth), depth), :]
        return down_ref.at[:, pl.ds(pl.multiple_of(shard * cols, cols), cols)]

    def w_copy(a, shard, kind, target, first=False, part=None):
        dst = slot(a, shard)
        src = own_part(a, half if part is None else part) if first else dst
        return remote(src, dst, w_send.at[a, kind, shard], w_recv.at[a, shard], target)

    for dz in range(1, NZ):
        @pl.when(z + dz < NZ)
        def _():
            for copy in kv_copies(sp, True, dz - 1, dev(z + dz, y, c)):
                copy.start()
    for kind, target in ((3, y_dev), (4, c_dev)):
        for copy in kv_copies(sp, True, kind, target):
            copy.start()

    for a in range(3):
        loads[a].wait()
        w_copy(a, sp, 0, dev(cross_in, y, c), True, 1 - half).start()
    for a in range(3):
        w_copy(a, sp, 1, m_dev, True).start()
        w_copy(a, sp, 3, c_dev, True).start()
    stores = [
        pltpu.make_async_copy(own_part(a, half), slot(a, sp), loc_out.at[a]) for a in range(3)
    ]
    for copy in stores:
        copy.start()

    lane_head = lax.broadcasted_iota(jnp.int32, (rows, width), 1) // HEAD_DIM
    q_all = q_ref[...].astype(jnp.float32) * HEAD_DIM ** (-0.5)
    for h in range(heads):
        qs[h] = jnp.where(lane_head == h, q_all, 0.0).astype(jnp.bfloat16)
    r_idx = lax.broadcasted_iota(jnp.int32, (rows, rows), 0)
    c_idx = lax.broadcasted_iota(jnp.int32, (rows, rows), 1)
    tri[...] = jnp.where(r_idx > c_idx, -1.0, 0.0).astype(jnp.bfloat16)
    acc[...] = jnp.zeros_like(acc)
    tail[...] = jnp.zeros_like(tail)

    def attend(kb, vb, masked):
        for h in range(heads):
            scores = lax.dot_general(
                qs[h], kb, (((1,), (1,)), ((), ())), preferred_element_type=jnp.float32
            ) - shift_ref[h]
            drop = jnp.maximum(scores, 0.0) + jnp.log(1.0 + jnp.exp(-jnp.abs(scores)))
            take = scores - drop
            if masked:
                drop = jnp.where(c_idx < r_idx, drop, 0.0)
            high = drop.astype(jnp.bfloat16)
            low = (drop - high.astype(jnp.float32)).astype(jnp.bfloat16)
            later = jnp.dot(high, tri[...], preferred_element_type=jnp.float32) + jnp.dot(
                low, tri[...], preferred_element_type=jnp.float32
            )
            before = tail[h]
            weights = jnp.exp(take + later + before[:, 0:1])
            if masked:
                weights = jnp.where(c_idx < r_idx, weights, 0.0)
            acc[h] += jnp.dot(weights.astype(jnp.bfloat16), vb, preferred_element_type=jnp.float32)
            tail[h] = before + (later[:, 0:1] - drop[:, 0:1])

    attend(k_ref[...], v_ref[...], True)

    for dz in range(1, NZ):
        @pl.when(z >= dz)
        def _():
            shard = dev(z - dz, y, c)
            for copy in kv_copies(shard, False, 3, y_dev):
                copy.wait_recv()
                copy.start()
            for copy in kv_copies(shard, False, 4, c_dev):
                copy.start()
        w_copy(dz - 1, sp, 2, y_dev, True).start()

    def plane(dz):
        for copy in kv_copies(dev(z - dz, 1 - y, c), False, 4, c_dev):
            copy.wait_recv()
            copy.start()
        for yy in (0, 1):
            for copy in kv_copies(dev(z - dz, yy, 1 - c), False, 4, c_dev):
                copy.wait_recv()
        in_plane = lax.rem(sp, NY * NC)
        if dz == 0:
            blocks(1, in_plane + 1)
        else:
            base = in_plane + (dz - 1) * NY * NC + 1
            blocks(base, base + NY * NC)

    def blocks(first, last):
        def body(i, carry):
            shard = sp - i
            attend(kv_slot(kbuf, shard)[...], kv_slot(vbuf, shard)[...], False)
            return carry

        lax.fori_loop(first, last, body, 0)

    def arrived(zz, to_mate):
        shard = dev(zz, y, c)
        for a in range(3):
            w_copy(a, shard, 1, m_dev).wait_recv()
            if to_mate:
                w_copy(a, shard, 1, m_dev).start()
            w_copy(a, shard, 2, y_dev).start()
            w_copy(a, shard, 3, c_dev).start()

    plane(0)
    @pl.when(inner)
    def _():
        arrived(cross_in, True)
    @pl.when(z >= 1)
    def _():
        plane(1)
    arrived(z_mate, False)
    @pl.when(z >= 2)
    def _():
        plane(2)
    @pl.when(inner)
    def _():
        arrived(cross_out, True)
    @pl.when(z >= 3)
    def _():
        arrived(cross_in, False)
        plane(3)

    total = jnp.zeros((rows, width), jnp.float32)
    for h in range(heads):
        total = jnp.where(lane_head == h, acc[h], total)
    att[...] = total.astype(jnp.bfloat16)

    own_rows = rows // 2
    there = pl.ds(pl.multiple_of((1 - tp) * own_rows, own_rows), own_rows)
    here = pl.ds(pl.multiple_of(tp * own_rows, own_rows), own_rows)
    swap = pltpu.make_async_remote_copy(
        src_ref=att.at[there, :], dst_ref=heads_in, send_sem=x_sem.at[0], recv_sem=x_sem.at[1],
        device_id={"tp": 1 - tp}, device_id_type=MESH,
    )
    swap.start()

    @pl.when(z == 0)
    def _():
        arrived(cross_in, False)

    out_rows = pl.ds(pl.multiple_of(tp * width, width), width)
    in_rows = pl.ds(pl.multiple_of((1 - tp) * width, width), width)
    wide = mixed.shape[1]
    step_cols = wide // 4
    for n in range(4):
        part = pl.ds(n * step_cols, step_cols)
        mixed[:, part] = jnp.dot(
            att[here, :], wo_ref[out_rows, part], preferred_element_type=jnp.float32
        )
    swap.wait_recv()
    for n in range(4):
        part = pl.ds(n * step_cols, step_cols)
        mixed[:, part] += jnp.dot(
            heads_in[...], wo_ref[in_rows, part], preferred_element_type=jnp.float32
        )

    @pl.loop(0, own_rows // 16)
    def _(i):
        part = pl.ds(pl.multiple_of(i * 16, 16), 16)
        value = mixed[part, :].astype(jnp.bfloat16).astype(jnp.float32)
        middle = (resid_ref[part, :].astype(jnp.float32) + mix_ref[...] * rms_scale(value)).astype(
            jnp.bfloat16
        )
        mid_ref[part, :] = middle
        normed[part, :] = (pre_ref[...] * rms_scale(middle.astype(jnp.float32))).astype(
            jnp.bfloat16
        )

    p_dev = dev(lax.rem(z + 2, NZ), y, c)

    def tok_slot(part, xx):
        first = (part * 2 + xx) * own_rows
        return tok_ref.at[pl.ds(pl.multiple_of(first, own_rows), own_rows), :]

    def tok_copy(src, part, xx, kind, target):
        return pltpu.make_async_remote_copy(
            src_ref=src, dst_ref=tok_slot(part, xx), send_sem=t_send.at[kind],
            recv_sem=t_recv.at[part, xx], device_id=target, device_id_type=MESH,
        )

    to_x = tok_copy(normed, half, tp, 0, {"tp": 1 - tp})
    to_p = tok_copy(normed, half, tp, 1, {"sp": p_dev})
    to_x.start()
    to_p.start()
    keep_own = pltpu.make_async_copy(normed, tok_slot(half, tp), x_sem.at[2])
    keep_own.start()
    relay = tok_copy(tok_slot(half, 1 - tp), half, 1 - tp, 2, {"sp": p_dev})
    relay.wait_recv()
    relay.start()

    @pl.when(jnp.logical_not(inner))
    def _():
        arrived(cross_out, False)
    for zz in (z, z_mate, cross_in, cross_out):
        for a in range(3):
            copy = w_copy(a, dev(zz, 1 - y, c), 3, c_dev)
            copy.wait_recv()
            copy.start()
    for zz in (z, z_mate, cross_in, cross_out):
        for yy in (y, 1 - y):
            for a in range(3):
                w_copy(a, dev(zz, yy, 1 - c), 3, c_dev).wait_recv()

    for xx in (tp, 1 - tp):
        tok_copy(normed, 1 - half, xx, 1, {"sp": p_dev}).wait_recv()

    for copy in (swap, to_x, to_p, relay):
        copy.wait_send()
    keep_own.wait()
    for copy in stores:
        copy.wait()
    for dz in range(1, NZ):
        @pl.when(z + dz < NZ)
        def _():
            for copy in kv_copies(sp, True, dz - 1, dev(z + dz, y, c)):
                copy.wait_send()
    for dz in range(NZ):
        @pl.when(z >= dz)
        def _():
            for copy in kv_copies(dev(z - dz, y, c), False, 3, y_dev):
                copy.wait_send()
            for yy in (y, 1 - y):
                for copy in kv_copies(dev(z - dz, yy, c), False, 4, c_dev):
                    copy.wait_send()
    for a in range(3):
        w_copy(a, sp, 0, m_dev).wait_send()
        w_copy(a, sp, 1, m_dev).wait_send()
        for zz in (z, z_mate, cross_in, cross_out):
            w_copy(a, dev(zz, y, c), 2, y_dev).wait_send()
            for yy in (y, 1 - y):
                w_copy(a, dev(zz, yy, c), 3, c_dev).wait_send()

    @pl.when(inner)
    def _():
        for zz in (cross_in, cross_out):
            for a in range(3):
                w_copy(a, dev(zz, y, c), 1, m_dev).wait_send()


def front(
    queries, keys, values, score_shift, resid, w_out, gain_mix, gain_pre, w_gate, w_up, w_down
):
    shards = lax.axis_size("sp")
    rows, width = queries.shape
    heads = width // HEAD_DIM
    depth, units = w_gate.shape[0], w_gate.shape[1] // 2
    cols = w_down.shape[1]
    vmem = pl.BlockSpec(memory_space=pltpu.VMEM)
    hbm = pl.BlockSpec(memory_space=pl.ANY)
    return pl.pallas_call(
        front_kernel,
        out_shape=(
            jax.ShapeDtypeStruct(resid.shape, jnp.bfloat16),
            jax.ShapeDtypeStruct((4 * resid.shape[0], resid.shape[1]), jnp.bfloat16),
            jax.ShapeDtypeStruct((shards * depth, units), jnp.bfloat16),
            jax.ShapeDtypeStruct((shards * depth, units), jnp.bfloat16),
            jax.ShapeDtypeStruct((units, shards * cols), jnp.bfloat16),
        ),
        in_specs=[vmem] * 3 + [pl.BlockSpec(memory_space=pltpu.SMEM)] + [vmem] * 4 + [hbm] * 3,
        out_specs=(vmem, hbm, hbm, hbm, hbm),
        scratch_shapes=[
            pltpu.VMEM((shards * rows, width), jnp.bfloat16),
            pltpu.VMEM((shards * rows, width), jnp.bfloat16),
            pltpu.VMEM((heads, rows, width), jnp.bfloat16),
            pltpu.VMEM((heads, rows, width), jnp.float32),
            pltpu.VMEM((heads, rows, 128), jnp.float32),
            pltpu.VMEM((rows, rows), jnp.bfloat16),
            pltpu.VMEM(w_gate.shape, jnp.bfloat16),
            pltpu.VMEM(w_up.shape, jnp.bfloat16),
            pltpu.VMEM(w_down.shape, jnp.bfloat16),
            pltpu.VMEM((rows, width), jnp.bfloat16),
            pltpu.VMEM((rows // 2, width), jnp.bfloat16),
            pltpu.VMEM(resid.shape, jnp.float32),
            pltpu.VMEM(resid.shape, jnp.bfloat16),
            pltpu.SemaphoreType.DMA((2, 5, shards)),
            pltpu.SemaphoreType.DMA((2, shards)),
            pltpu.SemaphoreType.DMA((3, 4, shards)),
            pltpu.SemaphoreType.DMA((3, shards)),
            pltpu.SemaphoreType.DMA((3,)),
            pltpu.SemaphoreType.DMA((3,)),
            pltpu.SemaphoreType.DMA((3,)),
            pltpu.SemaphoreType.DMA((3,)),
            pltpu.SemaphoreType.DMA((2, 2)),
        ],
        compiler_params=pltpu.CompilerParams(collective_id=0, has_side_effects=True),
        name="front",
    )(
        queries, keys, values, score_shift, resid, w_out, gain_mix[None], gain_pre[None],
        w_gate, w_up, w_down,
    )


def back_kernel(
    hid_ref, down_ref, mid_ref, post_ref, out_ref,
    own, out_x, in_x, out_z, in_z, x_send, x_recv, z_send, z_recv,
):
    rows, wide = mid_ref.shape
    parts = x_recv.shape[1]
    step_cols = wide // parts
    shards = NZ * NY * NC
    hop = shards // 2
    sp, tp = lax.axis_index("sp"), lax.axis_index("tp")
    half = sp // hop
    pair = lax.rem(sp + hop, shards)

    barrier = pltpu.get_barrier_semaphore()
    pl.semaphore_signal(barrier, inc=1, device_id={"tp": 1 - tp}, device_id_type=MESH)
    pl.semaphore_signal(barrier, inc=1, device_id={"sp": pair}, device_id_type=MESH)
    pl.semaphore_wait(barrier, 2)

    def block(part, xx):
        return hid_ref[pl.ds(pl.multiple_of((part * 2 + xx) * rows, rows), rows), :]

    def along_x(i, n):
        chunk = pl.ds(n * step_cols, step_cols)
        return pltpu.make_async_remote_copy(
            src_ref=out_x.at[i, :, chunk], dst_ref=in_x.at[i, :, chunk],
            send_sem=x_send.at[i, n], recv_sem=x_recv.at[i, n],
            device_id={"tp": 1 - tp}, device_id_type=MESH,
        )

    def along_z(n):
        chunk = pl.ds(n * step_cols, step_cols)
        return pltpu.make_async_remote_copy(
            src_ref=out_z.at[:, chunk], dst_ref=in_z.at[:, chunk],
            send_sem=z_send.at[n], recv_sem=z_recv.at[n],
            device_id={"sp": pair}, device_id_type=MESH,
        )

    def product(lhs, n):
        return jnp.dot(
            lhs, down_ref[:, n * step_cols : (n + 1) * step_cols],
            preferred_element_type=jnp.float32,
        ).astype(jnp.bfloat16)

    theirs = jnp.concatenate([block(1 - half, 1 - tp), block(half, 1 - tp)], axis=0)
    for n in range(parts):
        value = product(theirs, n)
        out_x[0, :, n * step_cols : (n + 1) * step_cols] = value[:rows]
        out_x[1, :, n * step_cols : (n + 1) * step_cols] = value[rows:]
        along_x(0, n).start()
    for n in range(parts):
        along_x(1, n).start()
    mine = jnp.concatenate([block(1 - half, tp), block(half, tp)], axis=0)
    for n in range(parts):
        value = product(mine, n)
        own[0, :, n * step_cols : (n + 1) * step_cols] = value[:rows]
        own[1, :, n * step_cols : (n + 1) * step_cols] = value[rows:]
    for n in range(parts):
        chunk = pl.ds(n * step_cols, step_cols)
        along_x(0, n).wait_recv()
        out_z[:, chunk] = (
            own[0, :, chunk].astype(jnp.float32) + in_x[0, :, chunk].astype(jnp.float32)
        ).astype(jnp.bfloat16)
        along_z(n).start()
    for n in range(parts):
        along_x(1, n).wait_recv()
    for n in range(parts):
        along_z(n).wait_recv()

    @pl.loop(0, rows // 16)
    def _(i):
        part = pl.ds(pl.multiple_of(i * 16, 16), 16)
        total = own[1, part, :].astype(jnp.float32) + in_x[1, part, :].astype(jnp.float32)
        total = (total + in_z[part, :].astype(jnp.float32)).astype(jnp.bfloat16)
        out_ref[part, :] = (
            mid_ref[part, :].astype(jnp.float32)
            + post_ref[...] * rms_scale(total.astype(jnp.float32))
        ).astype(jnp.bfloat16)

    for n in range(parts):
        along_x(0, n).wait_send()
        along_x(1, n).wait_send()
        along_z(n).wait_send()


def back(hidden, down_w, middle, gain_post):
    vmem = pl.BlockSpec(memory_space=pltpu.VMEM)
    parts = 4
    pair = pltpu.VMEM((2,) + middle.shape, jnp.bfloat16)
    one = pltpu.VMEM(middle.shape, jnp.bfloat16)
    return pl.pallas_call(
        back_kernel,
        out_shape=jax.ShapeDtypeStruct(middle.shape, jnp.bfloat16),
        in_specs=[vmem] * 4,
        out_specs=vmem,
        scratch_shapes=[
            pair, pair, pair, one, one,
            pltpu.SemaphoreType.DMA((2, parts)),
            pltpu.SemaphoreType.DMA((2, parts)),
            pltpu.SemaphoreType.DMA((parts,)),
            pltpu.SemaphoreType.DMA((parts,)),
        ],
        compiler_params=pltpu.CompilerParams(collective_id=1, has_side_effects=True),
        name="back",
    )(hidden, down_w, middle, gain_post[None])


def local(
    queries, keys, values, score_shift, resid, w_out, gain_mix, gain_pre,
    w_gate, w_up, conv_gate, conv_up, w_down, gain_post,
):
    middle, tokens, gate_w, up_w, down_w = front(
        queries, keys, values, score_shift, resid, w_out, gain_mix, gain_pre, w_gate, w_up, w_down
    )
    shards = lax.axis_size("sp")
    hop = shards // 2
    sp = lax.axis_index("sp")
    half = sp // hop
    units = gate_w.shape[1]
    run = tokens.shape[0] // 2
    conv_g = lax.dynamic_slice_in_dim(conv_gate, half * units, units, 1)
    conv_u = lax.dynamic_slice_in_dim(conv_up, half * units, units, 1)
    gate_part = jnp.dot(tokens, gate_w, preferred_element_type=jnp.float32).astype(jnp.bfloat16)
    up_part = jnp.dot(tokens, up_w, preferred_element_type=jnp.float32).astype(jnp.bfloat16)
    last = KERNEL - 1
    edges = jnp.stack(
        [
            jnp.stack([part[run - last : run], part[2 * run - last :]])
            for part in (gate_part, up_part)
        ]
    )
    ring = [(i, i // hop * hop + (i + 1) % hop) for i in range(shards)]
    before = lax.ppermute(edges, "sp", ring)
    first = sp % hop == 0
    before = jnp.where(
        first, jnp.stack([jnp.zeros_like(before[:, 0]), before[:, 0]], axis=1), before
    )

    def convolve(part, edge, taps):
        out = []
        for r in range(2):
            ext = jnp.concatenate([edge[r], part[r * run : (r + 1) * run]], 0).astype(jnp.float32)
            total = taps[0] * ext[0:run]
            for tap in range(1, KERNEL):
                total = total + taps[tap] * ext[tap : tap + run]
            out.append(total)
        return jnp.concatenate(out, 0)

    hidden = (
        jax.nn.silu(convolve(gate_part, before[0], conv_g)) * convolve(up_part, before[1], conv_u)
    ).astype(jnp.bfloat16)
    return back(hidden, down_w, middle, gain_post)


def solution(mesh):
    in_specs = (
        P("sp", "tp"),
        P("sp", "tp"),
        P("sp", "tp"),
        P("tp"),
        P(("sp", "tp"), None),
        P(),
        P(),
        P(),
        P("sp", "tp"),
        P("sp", "tp"),
        P(None, "tp"),
        P(None, "tp"),
        P("tp", "sp"),
        P(),
    )
    out_specs = P(("sp", "tp"), None)
    split = mesh.shape["sp"] == NZ * NY * NC and mesh.shape["tp"] == 2
    return jax.shard_map(local if split else generic_local, mesh=mesh, in_specs=in_specs, out_specs=out_specs, check_vma=False)
```
